256 devices in a mesh: fs: 32 (over z, y), tp: 8 (over x, core).
Axes of the slice: x: 4, y: 4, z: 8, core: 2. Of those that a mesh axis runs over, the one named last changes fastest.
Arguments:
- x_next: bfloat16 [6144, 2048], P(('fs', 'tp')), may hold values from -6 to 6
- x_prev: bfloat16 [6144, 2048], P(('fs', 'tp')), may hold values from -6 to 6
- grad_out: bfloat16 [6144, 2048], P(('fs', 'tp')), may hold values from -24 to 24
- gate_w: bfloat16 [2048, 2816], P('fs', 'tp'), may hold values from -0.125 to 0.125
- up_w: bfloat16 [2048, 2816], P('fs', 'tp'), may hold values from -0.125 to 0.125
- down_w: bfloat16 [2816, 2048], P('tp', 'fs'), may hold values from -0.109375 to 0.109375
- acc_gate: float32 [2048, 2816], P('fs', 'tp'), may hold values from -2.5 to 2.5
- acc_up: float32 [2048, 2816], P('fs', 'tp'), may hold values from -2.5 to 2.5
- acc_down: float32 [2816, 2048], P('tp', 'fs'), may hold values from -2.5 to 2.5
Outputs:
- out_next: bfloat16 [6144, 2048], P(('fs', 'tp'))
- saved_hidden: bfloat16 [6144, 2816], P('fs', 'tp')
- grad_input: bfloat16 [6144, 2048], P(('fs', 'tp'))
- new_gate: float32 [2048, 2816], P('fs', 'tp')
- new_up: float32 [2048, 2816], P('fs', 'tp')
- new_down: float32 [2816, 2048], P('tp', 'fs')
The draws below stay inside these ranges and needn't reach their ends.
All inputs are finite; a program needn't handle non-finite values.
Results may differ from the reference program's by a relative error of at most 0.014.
Values may be sent and summed in bfloat16 or wider, within the bound.
A program may use at most 64 MiB of HBM per device.

```python
import math
import jax
import jax.numpy as jnp
from jax import lax

D = 2048
FF = 2816
TOKENS = 6144
N_TP = 8


def spiked(drawn, rng, source, target, shards_of, factor):
    owner, partner = [(jnp.arange(drawn.shape[dim]) // (drawn.shape[dim] // shards_of)).reshape([-1 if axis == dim else 1 for axis in range(drawn.ndim)]) for dim in (source, target)]
    chosen = jax.random.permutation(rng, shards_of)[partner]
    strong = (owner == chosen) | (owner == (partner + shards_of // 2) % shards_of)
    return jnp.where(strong, factor * drawn, drawn)


def block_scale(key, extent, pieces, smallest, top_value):
    def one(axis_at, shards_of):
        draws = jax.random.uniform(jax.random.fold_in(jax.random.fold_in(key, 6), axis_at), (shards_of,), jnp.float32, smallest / len(pieces), top_value / len(pieces))
        return jnp.repeat(jnp.exp(draws), extent[axis_at] // shards_of).reshape((-1,) + (1,) * (len(extent) - axis_at - 1))

    loudness = one(*pieces[0])
    for cut in pieces[1:]:
        loudness = loudness * one(*cut)
    return loudness


def centred(own_key, dims, spread, bound, pieces=(), dtype=jnp.bfloat16):
    level = block_scale(own_key, dims, pieces, -0.22, 0.18) if pieces else 1.0
    entries = jax.random.normal(own_key, dims, jnp.float32) * spread * level
    return jnp.minimum(jnp.maximum(entries, -bound), bound).astype(dtype)


def heavy_noise(rng, shape, spread, limit, pieces, heavy, kind=jnp.bfloat16):
    entries = spread * jax.random.normal(rng, shape, jnp.float32)
    if pieces:
        entries = entries * block_scale(rng, shape, pieces, -0.22, 0.18)
    return jnp.clip(spiked(entries, jax.random.fold_in(rng, 3), *heavy), -limit, limit).astype(kind)


def setup_inputs(seed: int = 0) -> dict:
    key_list = jax.random.split(jax.random.key(seed), 10)
    return {
        "x_next": centred(key_list[0], (TOKENS, D), 1.0, 6.0, ((0, 256),)),
        "x_prev": centred(key_list[1], (TOKENS, D), 1.0, 6.0, ((0, 256),)),
        "grad_out": heavy_noise(key_list[2], (TOKENS, D), 1.0, 24.0, ((0, 256),), (0, 1, 256, 6.0)),
        "gate_w": centred(key_list[3], (D, FF), D ** -0.5, 0.125, ((0, 32), (1, 8))),
        "up_w": centred(key_list[4], (D, FF), D ** -0.5, 0.125, ((0, 32), (1, 8))),
        "down_w": centred(key_list[5], (FF, D), FF ** -0.5, 0.109375, ((0, 8), (1, 32))),
        "acc_gate": centred(key_list[6], (D, FF), 0.3, 2.5, ((0, 32), (1, 8)), jnp.float32),
        "acc_up": centred(key_list[7], (D, FF), 0.3, 2.5, ((0, 32), (1, 8)), jnp.float32),
        "acc_down": centred(key_list[8], (FF, D), 0.3, 2.5, ((0, 8), (1, 32)), jnp.float32),
    }


def block_sum(make_part):
    block = FF // N_TP
    total = None
    for index in range(N_TP):
        part = make_part(index * block, block)
        rounded = lax.optimization_barrier(part.astype(jnp.bfloat16)).astype(jnp.float32)
        total = rounded if total is None else total + rounded
    return total

def reference(x_next, x_prev, grad_out, gate_w, up_w, down_w, acc_gate, acc_up, acc_down):
    gate_next = jnp.dot(x_next, gate_w, preferred_element_type=jnp.float32)
    up_next = jnp.dot(x_next, up_w, preferred_element_type=jnp.float32)
    saved_hidden = (jax.nn.silu(gate_next) * up_next).astype(jnp.bfloat16)

    def out_part(start, width):
        return jnp.dot(saved_hidden[:, start:start + width], down_w[start:start + width], preferred_element_type=jnp.float32)
    out_next = block_sum(out_part).astype(jnp.bfloat16)
    gate_prev = jnp.dot(x_prev, gate_w, preferred_element_type=jnp.float32)
    up_prev = jnp.dot(x_prev, up_w, preferred_element_type=jnp.float32)
    grad_hidden = jnp.dot(grad_out, down_w.T, preferred_element_type=jnp.float32)
    sigmoid_gate = jax.nn.sigmoid(gate_prev)
    silu_gate = gate_prev * sigmoid_gate
    grad_gate = (grad_hidden * up_prev * sigmoid_gate * (1.0 + gate_prev * (1.0 - sigmoid_gate))).astype(jnp.bfloat16)
    grad_up = (grad_hidden * silu_gate).astype(jnp.bfloat16)
    hidden_prev = (silu_gate * up_prev).astype(jnp.bfloat16)

    def input_part(start, width):
        first = jnp.dot(grad_gate[:, start:start + width], gate_w[:, start:start + width].T, preferred_element_type=jnp.float32)
        second = jnp.dot(grad_up[:, start:start + width], up_w[:, start:start + width].T, preferred_element_type=jnp.float32)
        return first + second
    grad_input = block_sum(input_part).astype(jnp.bfloat16)
    factor = 1.0 / math.sqrt(TOKENS)
    new_gate = acc_gate + factor * jnp.dot(x_prev.T, grad_gate, preferred_element_type=jnp.float32)
    new_up = acc_up + factor * jnp.dot(x_prev.T, grad_up, preferred_element_type=jnp.float32)
    new_down = acc_down + factor * jnp.dot(hidden_prev.T, grad_out, preferred_element_type=jnp.float32)
    return (out_next, saved_hidden, grad_input, new_gate, new_up, new_down)
```

```python
import functools
import heapq
import math

import jax
import jax.numpy as jnp
from jax import lax
from jax.experimental import pallas as pl
from jax.experimental.pallas import tpu as pltpu
from jax.sharding import Mesh
from jax.sharding import PartitionSpec as P

MESH = pl.DeviceIdType.MESH
F32, BF16 = jnp.float32, jnp.bfloat16
TOK = ("z", "y", "x", "c")
FS, TP = ("z", "y"), ("x", "c")
NZ, NY, NX, NC = 8, 4, 4, 2
NB = NX * NC
ROWS, HALF = 64, 32
UNITS = 352
SEG = 384
WIDE = 3 * SEG
ZB = NY * ROWS
TOKENS = 24
GROUP = NB * TOKENS
LATE = 5
LATENCY, ROW_US = 1.8, 1.0 / 20.2

EZ = (0, 1, -1, 2, -2, 3, -3, 4)
EY = (0, 1, -1, 2)
REDUCE = (
    (4, 2), (3, 2), (-3, 2), (-2, 2), (4, -1), (4, 1), (3, -1), (-1, 2), (2, 2), (-3, -1), (3, 1), (-3, 1), (-2, -1),
    (1, 2), (-2, 1), (4, 0), (2, -1), (2, 1), (0, 2), (-3, 0), (3, 0), (-1, 1), (-1, -1), (-2, 0), (1, -1), (2, 0),
    (1, 1), (0, -1), (0, 1), (-1, 0), (1, 0),
)


def rows_of(m):
    ez, ey = m
    if abs(ey) == 2:
        return (0, HALF // 2) if ey > 0 else (HALF // 2, HALF)
    if ey == 0 and abs(ez) == 4:
        return (0, HALF // 2) if ez > 0 else (HALF // 2, HALF)
    return 0, HALF


def sends_of(n):
    ez, ey = n
    if abs(ey) == 1:
        return [(ez, 2 * ey)]
    if ey:
        return []
    along_y = [(ez, 1), (ez, -1)]
    if abs(ez) in (1, 2):
        return along_y + [(ez + (2 if ez > 0 else -2), 0)]
    return along_y


def node_of(m):
    ez, ey = m
    return (abs(ez) if ez == -4 else ez, abs(ey) if ey == -2 else ey)


def parts_of(n):
    ez, ey = n
    if ey == 2:
        return [(ez, 2), (ez, -2)]
    return [(4, 0), (-4, 0)] if n == (4, 0) else [n]


def step_of(m):
    ez, ey = m
    if ey:
        return "y", 1 if ey > 0 else -1
    return "z", (1 if abs(ez) == 1 else 2) * (1 if ez > 0 else -1)


@functools.lru_cache
def gather_plan():
    free, heap, got, order, ends = {}, [], set(), [], {}

    def push(now, m):
        axis, step = step_of(m)
        lo, hi = rows_of(m)
        cost = (hi - lo) * ROW_US * abs(step) if abs(m[0]) > 2 or m[1] else HALF * ROW_US * abs(step)
        link = axis, step > 0
        free[link] = max(now, free.get(link, 0.0)) + cost
        ends[m] = free[link]
        heapq.heappush(heap, (free[link] + LATENCY + 0.7 * (abs(step) - 1), len(ends), m))

    def issue(now, n):
        order.append((n, now))
        for m in sends_of(n):
            if m == (3, 0):
                push(now, (2, 0))
                push(now, (-2, 0))
            push(now, m)

    push(0.0, (1, 0))
    push(0.0, (-1, 0))
    issue(0.5, (0, 0))
    while heap:
        t, _, m = heapq.heappop(heap)
        got.add(m)
        if all(q in got for q in parts_of(node_of(m))):
            issue(t, node_of(m))
    ids = {m: i for i, m in enumerate(ends)}
    return order, ids


def layer(
    xn_in, xp_in, go_in, gw_in, uw_in, dw_in,
    out_ref, hid_ref, gin_ref, wg_out,
    mine, ours, own, w, tok, xpt, got, accp, accn, gg, hp, hid, hidv, gb, gr, s, r, far_sum, home_in, home,
    part, ring, ringed, plane, crossed, outv,
    ag_s, ag_r, home_s, home_r, twin_s, twin_r, hop_s, hop_r, tk_s, tk_r,
    gift_s, gift_r, rs_s, rs_r, top_s, top_r, back_s, back_r, ring_s, ring_r, plane_s, plane_r,
    hid_s, hid_r, out_s, in_s,
):
    z, y, x, c = (lax.axis_index(a) for a in ("z", "y", "x", "c"))
    par = lax.rem(z, 2)
    zp = z + 1 - 2 * par
    j = x * NC + c
    me = z * NY + y
    keeps = c == par
    moves = c != par
    size = {"z": NZ, "y": NY, "x": NX}
    here = {"z": z, "y": y, "x": x}

    def at(axis, step):
        return lax.rem(here[axis] + (step + size[axis]), size[axis])

    barrier = pltpu.get_barrier_semaphore()
    friends = [{"z": at("z", d), "c": q} for d in (1, -1, 2, -2) for q in range(NC)]
    friends += [{"y": at("y", 1)}, {"y": at("y", -1)}, {"x": at("x", 1)}, {"x": at("x", -1)}, {"c": 1 - c}]
    for friend in friends:
        pl.semaphore_signal(barrier, inc=1, device_id=friend, device_id_type=MESH)

    loads = [(ref, ours.at[i]) for i, ref in enumerate((gw_in, uw_in, dw_in))]
    loads += [(ref, mine.at[i]) for i, ref in enumerate((xp_in, go_in, xn_in))]
    loads = [pltpu.make_async_copy(src, dst, in_s.at[i]) for i, (src, dst) in enumerate(loads)]
    for copy in loads:
        copy.start()

    own[...] = jnp.zeros((NC, HALF, WIDE), BF16)
    for copy in loads:
        copy.wait()
    for q in range(NC):
        for i in range(3):
            own[q, :, SEG * i:SEG * i + UNITS] = ours[i, HALF * q:HALF * q + HALF, :]

    @pl.when(keeps)
    def _():
        w[me] = own[...]
        for a in range(3):
            tok[NB * a + j] = mine[a]

    with jax.named_scope("barrier"):
        pl.semaphore_wait(barrier, len(friends))

    def remote(src, dst, ssem, rsem, device):
        pltpu.make_async_remote_copy(
            src_ref=src, dst_ref=dst, send_sem=ssem, recv_sem=rsem, device_id=device, device_id_type=MESH
        ).start()

    def expect(dst, sem):
        pltpu.make_async_copy(dst, dst, sem).wait()

    order, ids = gather_plan()

    def chunk_at(n):
        return at("z", -n[0]) * NY + at("y", -n[1])

    def own_sends(step):
        for sign in (1, -1):
            for q in range(NC):
                remote(
                    own.at[q], w.at[me, q], top_s, ag_r.at[ids[(sign * step, 0)]],
                    {"z": at("z", sign * step), "c": q},
                )

    @pl.when(keeps)
    def _():
        remote(own, w.at[me], home_s, home_r, {"c": 1 - c})

    @pl.when(moves)
    def _():
        own_sends(1)

    @pl.when(moves)
    def _():
        for a in range(3):
            remote(mine.at[a], tok.at[NB * a + j], hop_s, hop_r.at[a, c], {"c": 1 - c})

    def hop(a):
        block = tok.at[NB * a + j]

        @pl.when(moves)
        def _():
            remote(mine.at[a], block, hop_s, hop_r.at[a, c], {"z": zp, "c": 1 - c})

        @pl.when(keeps)
        def _():
            remote(mine.at[a], block, hop_s, hop_r.at[a, c], {"z": zp})

    hop(0)

    @pl.when(moves)
    def _():
        expect(w.at[me], home_r)

    def forward(n):
        ch = chunk_at(n)
        for m in sends_of(n):
            if m == (3, 0):

                @pl.when(keeps)
                def _():
                    own_sends(2)

                hop(1)

            lo, hi = rows_of(m)
            piece = w.at[ch, c, pl.ds(lo, hi - lo)]
            axis, step = step_of(m)
            remote(piece, piece, ag_s, ag_r.at[ids[m]], {axis: at(axis, step)})
        if n != (0, 0):
            remote(w.at[ch, c], w.at[ch, c], twin_s, twin_r.at[EZ.index(n[0])], {"c": 1 - c})

    def tok_pair(a):
        pair = tok.at[pl.ds(NB * a + x * NC, NC)]
        for i, sign in enumerate((1, -1)):
            remote(pair, pair, tk_s, tk_r.at[a, i], {"x": at("x", sign)})

    def tok_stay(a):
        @pl.when(keeps)
        def _():
            expect(tok.at[NB * a + x * NC + 1 - c], hop_r.at[a, 1 - c])
            tok_pair(a)

    def tok_hop(a):
        @pl.when(moves)
        def _():
            for q in range(NC):
                expect(tok.at[NB * a + x * NC + q], hop_r.at[a, q])
            tok_pair(a)

    def tok_near(a, who):
        @pl.when(who)
        def _():
            for i, sign in enumerate((1, -1)):
                first = NB * a + at("x", -sign) * NC
                expect(tok.at[pl.ds(first, NC)], tk_r.at[a, i])
                block = tok.at[first + i]
                remote(block, block, tk_s, tk_r.at[a, 2 + i], {"x": at("x", sign)})

    def tok_far(a):
        for i in range(2):
            expect(tok.at[NB * a + at("x", 2) * NC + i], tk_r.at[a, 2 + i])

    def cols(zb):
        return pl.ds(pl.multiple_of(zb * ZB, ZB), ZB)

    def weights(zb):
        return w[pl.ds(zb * NY, NY)].reshape(ZB, WIDE)

    eye_zb = (
        lax.broadcasted_iota(jnp.int32, (ZB, ZB), 0) == lax.broadcasted_iota(jnp.int32, (ZB, ZB), 1)
    ).astype(BF16)

    def turn(a, dst, zb):
        block = tok[NB * a:NB * a + NB, :, cols(zb)].reshape(GROUP, ZB)
        dst[zb] = lax.dot_general(
            eye_zb, block, (((1,), (1,)), ((), ())), preferred_element_type=F32
        ).astype(BF16)

    def project(a, acc, lanes, zb, first):
        block = tok[NB * a:NB * a + NB, :, cols(zb)].reshape(GROUP, ZB)
        value = jnp.dot(block, weights(zb)[:, lanes[0]:lanes[1]], preferred_element_type=F32)
        if first:
            acc[:, lanes[0]:lanes[1]] = value
        else:
            acc[:, lanes[0]:lanes[1]] += value

    def block_steps(e):
        return (e,) if e in (0, 4) else (e, -e)

    done = set()
    turns = [functools.partial(turn, a, dst, at("z", -ez)) for a, dst in ((0, xpt), (1, got)) for ez in EZ[NZ - LATE:]]

    def project_block(a, e):
        for ez in block_steps(e):
            if ez not in twins:
                count = NY - 1 if ez == 0 else NY
                expect(w.at[pl.ds(0, count), 1 - c], twin_r.at[EZ.index(ez)])
                twins.add(ez)
            project(a, accp, ((0, 2 * SEG), (2 * SEG, WIDE))[a], at("z", -ez), ez == 0)
        done.add((a, e))

    twins, ready = set(), set()

    def fill(i):
        for a in range(2):
            for e in range(5):
                if a in ready and (a, e) not in done and i > last_of[e]:
                    project_block(a, e)
                    break
        for _ in range(2):
            if turns and (1 if len(turns) <= LATE else 0) in ready:
                turns.pop(0)()

    last_of = {
        e: max(i for i, (n, _) in enumerate(order) if abs(n[0]) == e) for e in range(5)
    }

    def tok_last(a):
        tok_far(a)
        ready.add(a)

    timed = [
        (1.0, tok_stay, 0), (1.1, tok_stay, 1), (6.4, tok_near, 0, keeps), (6.6, tok_hop, 0), (9.0, tok_near, 1, keeps),
        (9.1, hop, 2), (10.9, tok_hop, 1), (11.0, tok_near, 0, moves), (15.0, tok_near, 1, moves), (15.1, tok_stay, 2),
        (15.2, tok_hop, 2), (16.0, tok_last, 0), (19.7, tok_last, 1), (22.5, tok_near, 2, c >= 0),
    ]
    for i, (n, t) in enumerate(order):
        while timed and timed[0][0] <= (t if i + 1 < len(order) else 99):
            when, work, *given = timed.pop(0)
            with jax.named_scope("t#%s%.1f" % (work.__name__, when)):
                work(*given)
        with jax.named_scope("ga#i=%d#z=%d#y=%d" % (i, *n)):
            if n != (0, 0):
                for m in parts_of(n):
                    lo, hi = rows_of(m)
                    expect(w.at[chunk_at(n), c, pl.ds(lo, hi - lo)], ag_r.at[ids[m]])
            forward(n)
        if ready:
            with jax.named_scope("fill#i=%d" % i):
                fill(i)
    for work in turns:
        work()
    for e in range(5):
        for a in range(2):
            if (a, e) not in done:
                project_block(a, e)

    gate = accp[:, 0:SEG]
    upper = accp[:, SEG:2 * SEG]
    grad_h = accp[:, 2 * SEG:]
    sig = 1.0 / (1.0 + jnp.exp(-gate))
    silu = gate * sig
    gg[:, 0:SEG] = (grad_h * upper * sig * (1.0 + gate * (1.0 - sig))).astype(BF16)
    gg[:, SEG:] = (grad_h * silu).astype(BF16)
    hp[...] = (silu * upper).astype(BF16)

    def weight_grad(ez):
        zb = at("z", -ez)
        if ez in EZ[:NZ - LATE]:
            turn(0, xpt, zb)
            turn(1, got, zb)
        gb[zb, :, :, :, 0:2 * SEG] = jnp.dot(xpt[zb], gg[...], preferred_element_type=F32).astype(BF16).reshape(
            NY, NC, HALF, 2 * SEG
        )
        gb[zb, :, :, :, 2 * SEG:] = jnp.dot(got[zb], hp[...], preferred_element_type=F32).astype(BF16).reshape(
            NY, NC, HALF, SEG
        )
        remote(gb.at[zb, :, 1 - c], gr.at[zb], gift_s, gift_r.at[EZ.index(ez)], {"c": 1 - c})

    gifted = set()

    def add_up(n, store):
        ez, _ = n
        if ez not in gifted:
            expect(gr.at[at("z", -ez)], gift_r.at[EZ.index(ez)])
            gifted.add(ez)
        kids = [(m, rows_of(m)) for m in sends_of(n)]
        for m, (a, b) in kids:
            expect(r.at[m[0] + 4, m[1] + 2, pl.ds(a, b - a)], rs_r.at[ids[m]])
        edges = sorted({0, HALF, *(v for _, ab in kids for v in ab)})
        zb, yb = at("z", -ez), at("y", -n[1])
        for a, b in zip(edges, edges[1:]):
            total = gb[zb, yb, c, a:b, :].astype(F32) + gr[zb, yb, a:b, :].astype(F32)
            for m, (ka, kb) in kids:
                if ka <= a and b <= kb:
                    total = total + r[m[0] + 4, m[1] + 2, a:b, :].astype(F32)
            store(a, b, total)

    def give(n):
        sz, sy = n[0] + 4, n[1] + 2

        def store(a, b, total):
            s[sz, sy, a:b, :] = total.astype(BF16)

        add_up(n, store)
        for m in parts_of(n):
            a, b = rows_of(m)
            axis, step = step_of(m)
            piece = s.at[sz, sy, pl.ds(a, b - a)]
            if m[1] == 0 and abs(m[0]) <= 2:
                side = 0 if m[0] > 0 else 1
                remote(piece, far_sum.at[side, c], back_s, top_r.at[side, c], {"z": at("z", -step), "c": par})
            else:
                remote(
                    piece, r.at[m[0] + 4, m[1] + 2, pl.ds(a, b - a)], rs_s, rs_r.at[ids[m]],
                    {axis: at(axis, -step)},
                )

    outs = []

    def share(which, left, lanes, zb):
        value = lax.dot_general(
            left[...], w[zb * NY:zb * NY + NY].reshape(ZB, WIDE)[:, lanes[0]:lanes[1]],
            (((1,), (1,)), ((), ())), preferred_element_type=F32,
        ).astype(BF16).reshape(NB, TOKENS, ZB)
        part[which, :, :, ZB * zb:ZB * zb + ZB] = value
        if zb == NZ - 1:
            over, under, across = at("x", 1), at("x", -1), at("x", 2)
            for i, (block, to) in enumerate((
                (across * NC, over), (over * NC + 1, over), (across * NC + 1, under), (under * NC, under),
            )):
                remote(part.at[which, block], ring.at[which, i], ring_s, ring_r.at[which, i], {"x": to})

    def share_on(which):
        for i, (at_ring, sign) in enumerate(((0, 1), (2, -1))):
            to = at("x", sign)
            expect(ring.at[which, at_ring], ring_r.at[which, at_ring])
            ringed[which, i] = (
                part[which, to * NC + i].astype(F32) + ring[which, at_ring].astype(F32)
            ).astype(BF16)
            remote(ringed.at[which, i], ring.at[which, 4 + i], ring_s, ring_r.at[which, 4 + i], {"x": to})

    def share_plane(which):
        for i in (1, 3, 4, 5):
            expect(ring.at[which, i], ring_r.at[which, i])
        for q, (i, k) in enumerate(((3, 4), (1, 5))):
            plane[which, q] = (
                part[which, x * NC + q].astype(F32) + ring[which, i].astype(F32) + ring[which, k].astype(F32)
            ).astype(BF16)

        @pl.when(moves)
        def _():
            for q in range(NC):
                remote(plane.at[which, q], crossed.at[which, 0], plane_s, plane_r.at[which, 0], {"z": zp, "c": q})

        @pl.when(keeps)
        def _():
            remote(plane.at[which, 1 - c], crossed.at[which, 1], plane_s, plane_r.at[which, 1], {"c": 1 - c})

    def put(src, dst, i):
        pltpu.make_async_copy(src, dst, out_s.at[i]).start()

    def share_final(which, out):
        expect(crossed.at[which, 0], plane_r.at[which, 0])

        @pl.when(keeps)
        def _():
            outv[which] = (plane[which, c].astype(F32) + crossed[which, 0].astype(F32)).astype(BF16)

        @pl.when(moves)
        def _():
            expect(crossed.at[which, 1], plane_r.at[which, 1])
            outv[which] = (crossed[which, 1].astype(F32) + crossed[which, 0].astype(F32)).astype(BF16)

        put(outv.at[which], out, which)

    def forward_gate():
        gate = accn[:, 0:SEG]
        upper = accn[:, SEG:]
        value = (gate * (1.0 / (1.0 + jnp.exp(-gate))) * upper).astype(BF16)
        hid[...] = value

        @pl.when(keeps)
        def _():
            put(hid, hid_ref, 2)

        @pl.when(moves)
        def _():
            remote(hid, hidv, hid_s, hid_r, {"z": zp, "c": 1 - c})

    def hidden_out():
        @pl.when(moves)
        def _():
            expect(hidv, hid_r)
            put(hidv, hid_ref, 2)

    def next_blocks(ezs):
        for ez in ezs:
            project(2, accn, (0, 2 * SEG), at("z", -ez), ez == 0)

    def share_in(zb):
        share(1, gg, (0, 2 * SEG), zb)

    def share_next(zb):
        share(0, hid, (2 * SEG, WIDE), zb)

    plan = [(3 + i // 2, share_in, i) for i in range(NZ)]
    plan += [(7, tok_far, 2), (7, next_blocks, EZ[0:4]), (8, next_blocks, EZ[4:8]), (9, forward_gate)]
    plan += [(10 + i // 2, share_next, i) for i in range(NZ - 1)]
    plan += [
        (13, share_on, 1), (13, share_next, NZ - 1), (20, share_plane, 1), (23, share_on, 0), (26, hidden_out),
        (29, share_plane, 0), (92, share_final, 1, gin_ref), (93, share_final, 0, out_ref),
    ]

    def between(until):
        while plan and plan[0][0] <= until:
            _, work, *given = plan.pop(0)
            with jax.named_scope("w#%s" % "_".join([work.__name__] + [str(v) for v in given if isinstance(v, int)])):
                work(*given)

    graded = set()
    for count, n in enumerate(REDUCE):
        for e in (abs(n[0]), abs(n[0]) - 1):
            if e >= 0 and e not in graded:
                with jax.named_scope("wgrad#e=%d" % e):
                    for ez in block_steps(e):
                        weight_grad(ez)
                graded.add(e)
        with jax.named_scope("give#i=%d#z=%d#y=%d" % (count, *n)):
            give(n)
        between(count + 1)

    with jax.named_scope("last"):

        @pl.when(moves)
        def _():
            home[...] = jnp.zeros((NC, HALF, WIDE), F32)

        def keep(a, b, total):
            home_in[0, a:b, :] = total.astype(BF16)

            @pl.when(keeps)
            def _():
                home[c, a:b, :] = total

        add_up((0, 0), keep)

        @pl.when(moves)
        def _():
            remote(home_in.at[0], home_in.at[1], home_s, home_r, {"c": 1 - c})

    between(99)
    with jax.named_scope("final"):

        @pl.when(keeps)
        def _():
            expect(home_in.at[1], home_r)
            home[1 - c] = home_in[1].astype(F32)

        for side in range(2):
            for q in range(NC):
                expect(far_sum.at[side, q], top_r.at[side, q])
        for q in range(NC):
            home[q] = (
                home[q] + far_sum[0, q].astype(F32) + far_sum[1, q].astype(F32)
            )
        put(home, wg_out, 3)
    with jax.named_scope("drain"):
        routed = sum(rows_of(m)[1] - rows_of(m)[0] for m in ids if m[1] or abs(m[0]) > 2) // HALF
        for count, sem in ((routed, ag_s), (routed, rs_s), (4, top_s), (4, back_s), (NZ * NY - 1, twin_s)):
            expect(w.at[pl.ds(0, count), 0], sem)
        expect(gr, gift_s)
        for count, sem in ((18, tk_s), (12, ring_s)):
            expect(tok.at[pl.ds(0, count)], sem)

        @pl.when(keeps)
        def _():
            expect(own, home_s)
            expect(tok.at[pl.ds(0, 3)], hop_s)
            expect(tok.at[pl.ds(0, 2)], plane_s)

        @pl.when(moves)
        def _():
            expect(home_in.at[0], home_s)
            expect(tok.at[pl.ds(0, 6)], hop_s)
            expect(tok.at[pl.ds(0, 4)], plane_s)
            expect(hid, hid_s)

        for i, (src, dst) in enumerate(((outv.at[0], out_ref), (outv.at[1], gin_ref), (hid, hid_ref), (home, wg_out))):
            pltpu.make_async_copy(src, dst, out_s.at[i]).wait()


def finish(
    factor, out_in, hid_in, gin_in, wg_in, ag_in, au_in, ad_in,
    out_ref, hid_ref, gin_ref, ng_ref, nu_ref, nd_ref, hidv, wg, ag, au, ad, sems,
):
    pairs = ((wg_in, wg), (out_in, out_ref), (gin_in, gin_ref), (hid_in, hidv), (ag_in, ag), (au_in, au), (ad_in, ad))
    copies = [pltpu.make_async_copy(src, dst, sems.at[i]) for i, (src, dst) in enumerate(pairs)]
    for copy in copies:
        copy.start()
    for copy in copies:
        copy.wait()
    hid_ref[...] = hidv[:, 0:UNITS]
    for i, (acc, new) in enumerate(((ag, ng_ref), (au, nu_ref), (ad, nd_ref))):
        for q in range(NC):
            half = slice(HALF * q, HALF * q + HALF)
            new[half, :] = acc[half, :] + factor * wg[q, :, SEG * i:SEG * i + UNITS]


def local(x_next, x_prev, grad_out, gate_w, up_w, down_w, acc_gate, acc_up, acc_down):
    _, ids = gather_plan()
    vmem = pl.BlockSpec(memory_space=pltpu.VMEM)
    hbm = pl.BlockSpec(memory_space=pl.ANY)
    dma = pltpu.SemaphoreType.DMA
    total_rows = x_prev.shape[0] * NZ * NY * NX * NC
    factor = 1.0 / math.sqrt(total_rows)
    rows = jax.ShapeDtypeStruct((TOKENS, 2048), BF16)
    out_next, hidden, grad_input, grads = pl.pallas_call(
        layer,
        out_shape=(
            rows, jax.ShapeDtypeStruct((GROUP, SEG), BF16), rows, jax.ShapeDtypeStruct((NC, HALF, WIDE), F32),
        ),
        in_specs=[hbm] * 6,
        out_specs=(hbm,) * 4,
        scratch_shapes=[
            pltpu.VMEM((3, TOKENS, 2048), BF16),
            pltpu.VMEM((3, ROWS, UNITS), BF16),
            pltpu.VMEM((NC, HALF, WIDE), BF16),
            pltpu.VMEM((NZ * NY, NC, HALF, WIDE), BF16),
            pltpu.VMEM((3 * NB, TOKENS, 2048), BF16),
            pltpu.VMEM((NZ, ZB, GROUP), BF16),
            pltpu.VMEM((NZ, ZB, GROUP), BF16),
            pltpu.VMEM((GROUP, WIDE), F32),
            pltpu.VMEM((GROUP, 2 * SEG), F32),
            pltpu.VMEM((GROUP, 2 * SEG), BF16),
            pltpu.VMEM((GROUP, SEG), BF16),
            pltpu.VMEM((GROUP, SEG), BF16),
            pltpu.VMEM((GROUP, SEG), BF16),
            pltpu.VMEM((NZ, NY, NC, HALF, WIDE), BF16),
            pltpu.VMEM((NZ, NY, HALF, WIDE), BF16),
            pltpu.VMEM((9, 5, HALF, WIDE), BF16),
            pltpu.VMEM((9, 5, HALF, WIDE), BF16),
            pltpu.VMEM((2, NC, HALF, WIDE), BF16),
            pltpu.VMEM((2, HALF, WIDE), BF16),
            pltpu.VMEM((NC, HALF, WIDE), F32),
            pltpu.VMEM((2, NB, TOKENS, 2048), BF16),
            pltpu.VMEM((2, 6, TOKENS, 2048), BF16),
            pltpu.VMEM((2, 2, TOKENS, 2048), BF16),
            pltpu.VMEM((2, NC, TOKENS, 2048), BF16),
            pltpu.VMEM((2, NC, TOKENS, 2048), BF16),
            pltpu.VMEM((2, TOKENS, 2048), BF16),
            dma, dma((len(ids),)), dma, dma, dma, dma((len(EZ),)), dma, dma((3, NC)), dma, dma((3, 4)),
            dma, dma((len(EZ),)), dma, dma((len(ids),)), dma, dma((2, NC)), dma, dma,
            dma, dma((2, 6)), dma, dma((2, 2)),
            dma, dma, dma((4,)), dma((6,)),
        ],
        compiler_params=pltpu.CompilerParams(
            collective_id=0, has_side_effects=True, vmem_limit_bytes=60 * 1024 * 1024
        ),
        name="layer",
    )(x_next, x_prev, grad_out, gate_w, up_w, down_w.T)
    sums = jax.ShapeDtypeStruct((ROWS, UNITS), F32)
    out_next, hidden, grad_input, new_gate, new_up, new_down = pl.pallas_call(
        functools.partial(finish, factor),
        out_shape=(rows, jax.ShapeDtypeStruct((GROUP, UNITS), BF16), rows, sums, sums, sums),
        in_specs=[hbm] * 7,
        out_specs=(vmem,) * 6,
        scratch_shapes=[pltpu.VMEM((GROUP, SEG), BF16), pltpu.VMEM((NC, HALF, WIDE), F32)]
        + [pltpu.VMEM((ROWS, UNITS), F32)] * 3 + [dma((7,))],
        compiler_params=pltpu.CompilerParams(vmem_limit_bytes=60 * 1024 * 1024),
        name="finish",
    )(out_next, hidden, grad_input, grads, acc_gate, acc_up, acc_down.T)
    return out_next, hidden, grad_input, new_gate, new_up, new_down.T


def solution(mesh):
    split = Mesh(mesh.devices.reshape(NZ, NY, NX, NC), ("z", "y", "x", "c"))
    in_specs = (
        P(TOK, None), P(TOK, None), P(TOK, None),
        P(FS, TP), P(FS, TP), P(TP, FS), P(FS, TP), P(FS, TP), P(TP, FS),
    )
    out_specs = (P(TOK, None), P(FS, TP), P(TOK, None), P(FS, TP), P(FS, TP), P(TP, FS))
    return jax.shard_map(local, mesh=split, in_specs=in_specs, out_specs=out_specs, check_vma=False)
```

```python
import functools
import heapq
import math

import jax
import jax.numpy as jnp
from jax import lax
from jax.experimental import pallas as pl
from jax.experimental.pallas import tpu as pltpu
from jax.sharding import Mesh
from jax.sharding import PartitionSpec as P

MESH = pl.DeviceIdType.MESH
F32, BF16 = jnp.float32, jnp.bfloat16
TOK = ("z", "y", "x", "c")
FS, TP = ("z", "y"), ("x", "c")
NZ, NY, NX, NC = 8, 4, 4, 2
NB = NX * NC
PACK = 264
ROWS, HALF = 64, 32
UNITS = 352
SEG = 384
ZB = NY * ROWS
TOKENS = 24
GROUP = NB * TOKENS
LATE = 5
LATENCY, ROW_US = 1.8, 1.45 / 264

EZ = (0, 1, -1, 2, -2, 3, -3, 4)
EY = (0, 1, -1, 2)
REDUCE = (
    (4, 2), (3, 2), (-3, 2), (-2, 2), (2, 2), (4, -1), (4, 1), (-1, 2), (3, -1), (3, 1), (1, 2), (-3, -1), (-3, 1),
    (0, 2), (-2, -1), (-2, 1), (2, -1), (2, 1), (4, 0), (-1, -1), (-1, 1), (3, 0), (-3, 0), (1, -1), (1, 1), (0, -1),
    (0, 1), (-2, 0), (2, 0), (-1, 0), (1, 0),
)


def rows_of(m):
    ez, ey = m
    if abs(ey) == 2:
        return (0, 128) if ey > 0 else (128, PACK)
    if ey == 0 and abs(ez) == 4:
        return (0, 128) if ez > 0 else (128, PACK)
    return 0, PACK


def sends_of(n):
    ez, ey = n
    if abs(ey) == 1:
        return [(ez, 2 * ey)]
    if ey:
        return []
    along_y = [(ez, 1), (ez, -1)]
    if abs(ez) in (1, 2):
        return along_y + [(ez + (2 if ez > 0 else -2), 0)]
    return along_y


def node_of(m):
    ez, ey = m
    return (abs(ez) if ez == -4 else ez, abs(ey) if ey == -2 else ey)


def parts_of(n):
    ez, ey = n
    if ey == 2:
        return [(ez, 2), (ez, -2)]
    return [(4, 0), (-4, 0)] if n == (4, 0) else [n]


def step_of(m):
    ez, ey = m
    if ey:
        return "y", 1 if ey > 0 else -1
    return "z", (1 if abs(ez) == 1 else 2) * (1 if ez > 0 else -1)


def widened(v, lanes):
    return jnp.concatenate([v, jnp.zeros((v.shape[0], lanes - v.shape[1]), v.dtype)], axis=1)


def known(v):
    v = v[:, 0:SEG]
    return jnp.where(lax.broadcasted_iota(jnp.int32, v.shape, 1) < UNITS, v, 0.0)


def packed_pair(gate, upper):
    both = pltpu.roll(widened(upper, 512), 96, 1)
    return jnp.concatenate([gate[:, 0:256], gate[:, 256:384] + both[:, 0:128], both[:, 128:512]], axis=1)


def packed_last(down):
    return pltpu.roll(widened(down, 512), 64, 1)


def folded(v):
    v = v.reshape(v.shape[0] // HALF, 4, 8, 128)
    total = v[:, 0].reshape(-1, 128)
    for k in range(1, 4):
        total = total + pltpu.roll(v[:, k].reshape(-1, 128), 32 * k, 1)
    return total


def unfolded(v):
    n = v.shape[0] // 8
    keep = lax.broadcasted_iota(jnp.int32, v.shape, 1) < 32
    parts = [jnp.where(keep, v if k == 0 else pltpu.roll(v, 128 - 32 * k, 1), 0.0).reshape(n, 1, 8, 128) for k in range(4)]
    return jnp.concatenate(parts, axis=1).reshape(HALF * n, 128)


@functools.lru_cache
def gather_plan():
    free, heap, got, order, ends = {}, [], set(), [], {}

    def push(now, m):
        axis, step = step_of(m)
        lo, hi = rows_of(m)
        cost = (hi - lo) * ROW_US * abs(step) if abs(m[0]) > 2 or m[1] else PACK * ROW_US * abs(step)
        link = axis, step > 0
        free[link] = max(now, free.get(link, 0.0)) + cost
        ends[m] = free[link]
        heapq.heappush(heap, (free[link] + LATENCY + 0.7 * (abs(step) - 1), len(ends), m))

    def issue(now, n):
        order.append((n, now))
        for m in sends_of(n):
            if m == (3, 0):
                push(now, (2, 0))
                push(now, (-2, 0))
            push(now, m)

    push(0.0, (1, 0))
    push(0.0, (-1, 0))
    issue(0.5, (0, 0))
    while heap:
        t, _, m = heapq.heappop(heap)
        got.add(m)
        if all(q in got for q in parts_of(node_of(m))):
            issue(t, node_of(m))
    ids = {m: i for i, m in enumerate(ends)}
    return order, ids


def layer(
    xn_in, xp_in, go_in, gw_in, uw_in, dw_in,
    out_ref, hid_ref, gin_ref, wg_out,
    mine, ours, own, w, tok, xpt, got, accp, accd, accn, gg, hp, hid, hidp, hidv, gb, gr, s, r, far_sum, home_in, home,
    part, ring, ringed, plane, crossed, outv,
    ag_s, ag_r, home_s, home_r, twin_s, twin_r, hop_s, hop_r, tk_s, tk_r,
    gift_s, gift_r, rs_s, rs_r, top_s, top_r, back_s, back_r, ring_s, ring_r, plane_s, plane_r,
    hid_s, hid_r, out_s, in_s,
):
    z, y, x, c = (lax.axis_index(a) for a in ("z", "y", "x", "c"))
    par = lax.rem(z, 2)
    zp = z + 1 - 2 * par
    j = x * NC + c
    me = z * NY + y
    keeps = c == par
    moves = c != par
    size = {"z": NZ, "y": NY, "x": NX}
    here = {"z": z, "y": y, "x": x}

    def at(axis, step):
        return lax.rem(here[axis] + (step + size[axis]), size[axis])

    barrier = pltpu.get_barrier_semaphore()
    friends = [{"z": at("z", d), "c": q} for d in (1, -1, 2, -2) for q in range(NC)]
    friends += [{"y": at("y", 1)}, {"y": at("y", -1)}, {"x": at("x", 1)}, {"x": at("x", -1)}, {"c": 1 - c}]
    for friend in friends:
        pl.semaphore_signal(barrier, inc=1, device_id=friend, device_id_type=MESH)

    loads = [(ref, ours.at[i]) for i, ref in enumerate((gw_in, uw_in, dw_in))]
    loads += [(ref, mine.at[i]) for i, ref in enumerate((xp_in, go_in, xn_in))]
    loads = [pltpu.make_async_copy(src, dst, in_s.at[i]) for i, (src, dst) in enumerate(loads)]
    for copy in loads:
        copy.start()

    for copy in loads:
        copy.wait()

    gate_up_down = [widened(ours[i].astype(F32), SEG) for i in range(3)]
    pair = packed_pair(*gate_up_down[0:2])
    last = packed_last(gate_up_down[2])
    for q in range(NC):
        rows = slice(HALF * q, HALF * q + HALF)
        for t in range(8):
            column = jnp.zeros((HALF, 128), F32)
            if t < 6:
                column = column + pair[rows, 128 * t:128 * t + 128]
            if t > 4:
                column = column + last[rows, 128 * (t - 5):128 * (t - 4)]
            own[q, HALF * t:HALF * t + HALF, :] = column.astype(BF16)
        own[q, 256:PACK, :] = folded(last[rows, 384:512]).astype(BF16)

    @pl.when(keeps)
    def _():
        w[me] = own[...]
        for a in range(3):
            tok[NB * a + j] = mine[a]

    with jax.named_scope("barrier"):
        pl.semaphore_wait(barrier, len(friends))

    def remote(src, dst, ssem, rsem, device):
        pltpu.make_async_remote_copy(
            src_ref=src, dst_ref=dst, send_sem=ssem, recv_sem=rsem, device_id=device, device_id_type=MESH
        ).start()

    def expect(dst, sem):
        pltpu.make_async_copy(dst, dst, sem).wait()

    order, ids = gather_plan()

    def chunk_at(n):
        return at("z", -n[0]) * NY + at("y", -n[1])

    def own_sends(step):
        for sign in (1, -1):
            for q in range(NC):
                remote(
                    own.at[q], w.at[me, q], top_s, ag_r.at[ids[(sign * step, 0)]],
                    {"z": at("z", sign * step), "c": q},
                )

    @pl.when(keeps)
    def _():
        remote(own, w.at[me], home_s, home_r, {"c": 1 - c})

    @pl.when(moves)
    def _():
        own_sends(1)

    @pl.when(moves)
    def _():
        for a in range(3):
            remote(mine.at[a], tok.at[NB * a + j], hop_s, hop_r.at[a, c], {"c": 1 - c})

    def hop(a):
        block = tok.at[NB * a + j]

        @pl.when(moves)
        def _():
            remote(mine.at[a], block, hop_s, hop_r.at[a, c], {"z": zp, "c": 1 - c})

        @pl.when(keeps)
        def _():
            remote(mine.at[a], block, hop_s, hop_r.at[a, c], {"z": zp})

    hop(0)

    @pl.when(moves)
    def _():
        expect(w.at[me], home_r)

    def forward(n):
        ch = chunk_at(n)
        for m in sends_of(n):
            if m == (3, 0):

                @pl.when(keeps)
                def _():
                    own_sends(2)

                hop(1)

            lo, hi = rows_of(m)
            piece = w.at[ch, c, pl.ds(lo, hi - lo)]
            axis, step = step_of(m)
            remote(piece, piece, ag_s, ag_r.at[ids[m]], {axis: at(axis, step)})
        if n != (0, 0):
            remote(w.at[ch, c], w.at[ch, c], twin_s, twin_r.at[EZ.index(n[0])], {"c": 1 - c})

    def tok_pair(a):
        pair = tok.at[pl.ds(NB * a + x * NC, NC)]
        for i, sign in enumerate((1, -1)):
            remote(pair, pair, tk_s, tk_r.at[a, i], {"x": at("x", sign)})

    def tok_stay(a):
        @pl.when(keeps)
        def _():
            expect(tok.at[NB * a + x * NC + 1 - c], hop_r.at[a, 1 - c])
            tok_pair(a)

    def tok_hop(a):
        @pl.when(moves)
        def _():
            for q in range(NC):
                expect(tok.at[NB * a + x * NC + q], hop_r.at[a, q])
            tok_pair(a)

    def tok_near(a, who):
        @pl.when(who)
        def _():
            for i, sign in enumerate((1, -1)):
                first = NB * a + at("x", -sign) * NC
                expect(tok.at[pl.ds(first, NC)], tk_r.at[a, i])
                block = tok.at[first + i]
                remote(block, block, tk_s, tk_r.at[a, 2 + i], {"x": at("x", sign)})

    def tok_far(a):
        for i in range(2):
            expect(tok.at[NB * a + at("x", 2) * NC + i], tk_r.at[a, 2 + i])

    def cols(zb):
        return pl.ds(pl.multiple_of(zb * ZB, ZB), ZB)

    def weights(zb, first, end):
        parts = [w[pl.ds(zb * NY, NY), :, HALF * t:HALF * t + HALF, :].reshape(ZB, 128) for t in range(first, min(end, 8))]
        if end > 8:
            tail = w[pl.ds(zb * NY, NY), :, 256:PACK, :].astype(F32).reshape(NY * NC * 8, 128)
            parts.append(unfolded(tail).astype(BF16))
        return jnp.concatenate(parts, axis=1)

    eye_zb = (
        lax.broadcasted_iota(jnp.int32, (ZB, ZB), 0) == lax.broadcasted_iota(jnp.int32, (ZB, ZB), 1)
    ).astype(BF16)

    def turn(a, dst, zb):
        block = tok[NB * a:NB * a + NB, :, cols(zb)].reshape(GROUP, ZB)
        dst[zb] = lax.dot_general(
            eye_zb, block, (((1,), (1,)), ((), ())), preferred_element_type=F32
        ).astype(BF16)

    def project(a, acc, columns, zb, first):
        block = tok[NB * a:NB * a + NB, :, cols(zb)].reshape(GROUP, ZB)
        value = jnp.dot(block, weights(zb, *columns), preferred_element_type=F32)
        if first:
            acc[...] = value
        else:
            acc[...] += value

    def block_steps(e):
        return (e,) if e in (0, 4) else (e, -e)

    done = set()
    turns = [functools.partial(turn, a, dst, at("z", -ez)) for a, dst in ((0, xpt), (1, got)) for ez in EZ[NZ - LATE:]]

    def project_block(a, e):
        for ez in block_steps(e):
            if ez not in twins:
                count = NY - 1 if ez == 0 else NY
                expect(w.at[pl.ds(0, count), 1 - c], twin_r.at[EZ.index(ez)])
                twins.add(ez)
            project(a, (accp, accd)[a], ((0, 6), (5, 9))[a], at("z", -ez), ez == 0)
        done.add((a, e))

    twins, ready = set(), set()

    def fill(i):
        for a in range(2):
            for e in range(5):
                if a in ready and (a, e) not in done and i > last_of[e]:
                    project_block(a, e)
                    break
        for _ in range(2):
            if turns and (1 if len(turns) <= LATE else 0) in ready:
                turns.pop(0)()

    last_of = {
        e: max(i for i, (n, _) in enumerate(order) if abs(n[0]) == e) for e in range(5)
    }

    def tok_last(a):
        tok_far(a)
        ready.add(a)

    timed = [
        (1.0, tok_stay, 0), (1.1, tok_stay, 1), (6.4, tok_near, 0, keeps), (6.6, tok_hop, 0), (9.0, tok_near, 1, keeps),
        (9.1, hop, 2), (10.9, tok_hop, 1), (11.0, tok_near, 0, moves), (15.0, tok_near, 1, moves), (15.1, tok_stay, 2),
        (15.2, tok_hop, 2), (16.0, tok_last, 0), (19.7, tok_last, 1), (22.5, tok_near, 2, c >= 0),
    ]
    for i, (n, t) in enumerate(order):
        while timed and timed[0][0] <= (t if i + 1 < len(order) else 99):
            when, work, *given = timed.pop(0)
            with jax.named_scope("t#%s%.1f" % (work.__name__, when)):
                work(*given)
        with jax.named_scope("ga#i=%d#z=%d#y=%d" % (i, *n)):
            if n != (0, 0):
                for m in parts_of(n):
                    lo, hi = rows_of(m)
                    expect(w.at[chunk_at(n), c, pl.ds(lo, hi - lo)], ag_r.at[ids[m]])
            forward(n)
        if ready:
            with jax.named_scope("fill#i=%d" % i):
                fill(i)
    for work in turns:
        work()
    for e in range(5):
        for a in range(2):
            if (a, e) not in done:
                project_block(a, e)

    gate = known(accp[...])
    upper = known(pltpu.roll(accp[...], 768 - UNITS, 1))
    grad_h = known(pltpu.roll(accd[...], 448, 1))
    sig = 1.0 / (1.0 + jnp.exp(-gate))
    silu = gate * sig
    gg[...] = packed_pair(
        grad_h * upper * sig * (1.0 + gate * (1.0 - sig)), grad_h * silu
    ).astype(BF16)
    hp[...] = packed_last(silu * upper).astype(BF16)

    def weight_grad(ez):
        zb = at("z", -ez)
        if ez in EZ[:NZ - LATE]:
            turn(0, xpt, zb)
            turn(1, got, zb)
        pair = jnp.dot(xpt[zb], gg[...], preferred_element_type=F32)
        last = jnp.dot(got[zb], hp[...], preferred_element_type=F32)
        for t in range(8):
            if t < 5:
                column = pair[:, 128 * t:128 * t + 128]
            elif t == 5:
                column = pair[:, 640:768] + last[:, 0:128]
            else:
                column = last[:, 128 * (t - 5):128 * (t - 4)]
            gb[zb, :, :, HALF * t:HALF * t + HALF, :] = column.astype(BF16).reshape(NY, NC, HALF, 128)
        gb[zb, :, :, 256:PACK, :] = folded(last[:, 384:512]).astype(BF16).reshape(NY, NC, 8, 128)
        remote(gb.at[zb, :, 1 - c], gr.at[zb], gift_s, gift_r.at[EZ.index(ez)], {"c": 1 - c})

    gifted = set()

    def add_up(n, store):
        ez, _ = n
        if ez not in gifted:
            expect(gr.at[at("z", -ez)], gift_r.at[EZ.index(ez)])
            gifted.add(ez)
        kids = [(m, rows_of(m)) for m in sends_of(n)]
        for m, (a, b) in kids:
            expect(r.at[m[0] + 4, m[1] + 2, pl.ds(a, b - a)], rs_r.at[ids[m]])
        edges = sorted({0, PACK, *(v for _, ab in kids for v in ab)})
        zb, yb = at("z", -ez), at("y", -n[1])
        for a, b in zip(edges, edges[1:]):
            total = gb[zb, yb, c, a:b, :].astype(F32) + gr[zb, yb, a:b, :].astype(F32)
            for m, (ka, kb) in kids:
                if ka <= a and b <= kb:
                    total = total + r[m[0] + 4, m[1] + 2, a:b, :].astype(F32)
            store(a, b, total)

    def give(n):
        sz, sy = n[0] + 4, n[1] + 2

        def store(a, b, total):
            s[sz, sy, a:b, :] = total.astype(BF16)

        add_up(n, store)
        for m in parts_of(n):
            a, b = rows_of(m)
            axis, step = step_of(m)
            piece = s.at[sz, sy, pl.ds(a, b - a)]
            if m[1] == 0 and abs(m[0]) <= 2:
                side = 0 if m[0] > 0 else 1
                remote(piece, far_sum.at[side, c], back_s, top_r.at[side, c], {"z": at("z", -step), "c": par})
            else:
                remote(
                    piece, r.at[m[0] + 4, m[1] + 2, pl.ds(a, b - a)], rs_s, rs_r.at[ids[m]],
                    {axis: at(axis, -step)},
                )

    outs = []

    def share(which, left, columns, zb):
        value = lax.dot_general(
            left[...], weights(zb, *columns),
            (((1,), (1,)), ((), ())), preferred_element_type=F32,
        ).astype(BF16).reshape(NB, TOKENS, ZB)
        part[which, :, :, ZB * zb:ZB * zb + ZB] = value
        if zb % 4 == 3:
            h = zb // 4
            over, under, across = at("x", 1), at("x", -1), at("x", 2)
            for i, (block, to) in enumerate((
                (across * NC, over), (over * NC + 1, over), (across * NC + 1, under), (under * NC, under),
            )):
                remote(
                    part.at[which, block, :, wide[h]], ring.at[which, i, :, wide[h]],
                    ring_s, ring_r.at[which, h, i], {"x": to},
                )

    wide = (pl.ds(0, 1024), pl.ds(1024, 1024))

    def share_on(which, h):
        for i, (at_ring, sign) in enumerate(((0, 1), (2, -1))):
            to = at("x", sign)
            expect(ring.at[which, at_ring, :, wide[h]], ring_r.at[which, h, at_ring])
            ringed[which, i, :, wide[h]] = (
                part[which, to * NC + i, :, wide[h]].astype(F32) + ring[which, at_ring, :, wide[h]].astype(F32)
            ).astype(BF16)
            remote(
                ringed.at[which, i, :, wide[h]], ring.at[which, 4 + i, :, wide[h]],
                ring_s, ring_r.at[which, h, 4 + i], {"x": to},
            )

    def share_plane(which, h):
        for i in (1, 3, 4, 5):
            expect(ring.at[which, i, :, wide[h]], ring_r.at[which, h, i])
        for q, (i, k) in enumerate(((3, 4), (1, 5))):
            plane[which, q, :, wide[h]] = (
                part[which, x * NC + q, :, wide[h]].astype(F32)
                + ring[which, i, :, wide[h]].astype(F32) + ring[which, k, :, wide[h]].astype(F32)
            ).astype(BF16)

        @pl.when(moves)
        def _():
            for q in range(NC):
                remote(
                    plane.at[which, q, :, wide[h]], crossed.at[which, 0, :, wide[h]],
                    plane_s, plane_r.at[which, h, 0], {"z": zp, "c": q},
                )

        @pl.when(keeps)
        def _():
            remote(
                plane.at[which, 1 - c, :, wide[h]], crossed.at[which, 1, :, wide[h]],
                plane_s, plane_r.at[which, h, 1], {"c": 1 - c},
            )

    def put(src, dst, i):
        pltpu.make_async_copy(src, dst, out_s.at[i]).start()

    def share_final(which, out):
        for h in range(2):
            expect(crossed.at[which, 0, :, wide[h]], plane_r.at[which, h, 0])

        @pl.when(keeps)
        def _():
            outv[which] = (plane[which, c].astype(F32) + crossed[which, 0].astype(F32)).astype(BF16)

        @pl.when(moves)
        def _():
            for h in range(2):
                expect(crossed.at[which, 1, :, wide[h]], plane_r.at[which, h, 1])
            outv[which] = (crossed[which, 1].astype(F32) + crossed[which, 0].astype(F32)).astype(BF16)

        put(outv.at[which], out, which)

    def forward_gate():
        gate = known(accn[...])
        upper = known(pltpu.roll(accn[...], 768 - UNITS, 1))
        value = gate * (1.0 / (1.0 + jnp.exp(-gate))) * upper
        hid[...] = value.astype(BF16)
        hidp[...] = packed_last(value).astype(BF16)

        @pl.when(keeps)
        def _():
            put(hid, hid_ref, 2)

        @pl.when(moves)
        def _():
            remote(hid, hidv, hid_s, hid_r, {"z": zp, "c": 1 - c})

    def hidden_out():
        @pl.when(moves)
        def _():
            expect(hidv, hid_r)
            put(hidv, hid_ref, 2)

    def next_blocks(ezs):
        for ez in ezs:
            project(2, accn, (0, 6), at("z", -ez), ez == 0)

    def share_in(zb):
        share(1, gg, (0, 6), zb)

    def share_next(zb):
        share(0, hidp, (5, 9), zb)

    plan = [(0, share_in, 0)] + [(3 + (i - 1) // 2, share_in, i) for i in range(1, NZ)]
    plan += [(7, tok_far, 2), (7, next_blocks, EZ[0:4]), (8, next_blocks, EZ[4:8]), (9, forward_gate)]
    plan += [(9, share_next, 0), (9, share_on, 1, 0), (10, share_next, 1), (10, share_next, 2), (11, share_next, 3)]
    plan += [(11, share_next, 4), (12, share_next, 5), (12, share_on, 1, 1), (13, share_next, 6), (13, share_next, 7)]
    plan += [
        (19, share_plane, 1, 0), (22, share_on, 0, 0), (23, share_plane, 1, 1), (26, share_on, 0, 1),
        (27, hidden_out), (28, share_plane, 0, 0), (29, share_plane, 0, 1),
        (92, share_final, 1, gin_ref), (93, share_final, 0, out_ref),
    ]

    def between(until):
        while plan and plan[0][0] <= until:
            _, work, *given = plan.pop(0)
            with jax.named_scope("w#%s" % "_".join([work.__name__] + [str(v) for v in given if isinstance(v, int)])):
                work(*given)

    graded = set()
    for count, n in enumerate(REDUCE):
        for e in (abs(n[0]), abs(n[0]) - 1):
            if e >= 0 and e not in graded:
                with jax.named_scope("wgrad#e=%d" % e):
                    for ez in block_steps(e):
                        weight_grad(ez)
                graded.add(e)
        between(count)
        with jax.named_scope("give#i=%d#z=%d#y=%d" % (count, *n)):
            give(n)
        between(count + 1)

    with jax.named_scope("last"):

        @pl.when(moves)
        def _():
            home[...] = jnp.zeros((NC, PACK, 128), F32)

        def keep(a, b, total):
            home_in[0, a:b, :] = total.astype(BF16)

            @pl.when(keeps)
            def _():
                home[c, a:b, :] = total

        add_up((0, 0), keep)

        @pl.when(moves)
        def _():
            remote(home_in.at[0], home_in.at[1], home_s, home_r, {"c": 1 - c})

    between(99)
    with jax.named_scope("final"):

        @pl.when(keeps)
        def _():
            expect(home_in.at[1], home_r)
            home[1 - c] = home_in[1].astype(F32)

        for side in range(2):
            for q in range(NC):
                expect(far_sum.at[side, q], top_r.at[side, q])
        for q in range(NC):
            home[q] = (
                home[q] + far_sum[0, q].astype(F32) + far_sum[1, q].astype(F32)
            )
        put(home, wg_out, 3)
    with jax.named_scope("drain"):
        routed = sum(rows_of(m)[1] - rows_of(m)[0] for m in ids if m[1] or abs(m[0]) > 2) // PACK
        for count, sem in ((routed, ag_s), (routed, rs_s), (4, top_s), (4, back_s), (NZ * NY - 1, twin_s)):
            expect(w.at[pl.ds(0, count), 0], sem)
        expect(gr, gift_s)
        for count, sem in ((18, tk_s), (12, ring_s)):
            expect(tok.at[pl.ds(0, count)], sem)

        @pl.when(keeps)
        def _():
            expect(own, home_s)
            expect(tok.at[pl.ds(0, 3)], hop_s)
            expect(tok.at[pl.ds(0, 2)], plane_s)

        @pl.when(moves)
        def _():
            expect(home_in.at[0], home_s)
            expect(tok.at[pl.ds(0, 6)], hop_s)
            expect(tok.at[pl.ds(0, 4)], plane_s)
            expect(hid, hid_s)

        for i, (src, dst) in enumerate(((outv.at[0], out_ref), (outv.at[1], gin_ref), (hid, hid_ref), (home, wg_out))):
            pltpu.make_async_copy(src, dst, out_s.at[i]).wait()


def finish(
    factor, out_in, hid_in, gin_in, wg_in, ag_in, au_in, ad_in,
    out_ref, hid_ref, gin_ref, ng_ref, nu_ref, nd_ref, hidv, wg, ag, au, ad, sems,
):
    pairs = ((wg_in, wg), (out_in, out_ref), (gin_in, gin_ref), (hid_in, hidv), (ag_in, ag), (au_in, au), (ad_in, ad))
    copies = [pltpu.make_async_copy(src, dst, sems.at[i]) for i, (src, dst) in enumerate(pairs)]
    for copy in copies:
        copy.start()
    for copy in copies:
        copy.wait()
    hid_ref[...] = hidv[:, 0:UNITS]
    for q in range(NC):
        column = [wg[q, HALF * t:HALF * t + HALF, :] for t in range(8)]
        tail = unfolded(wg[q, 256:PACK, :])
        gate = jnp.concatenate(column[0:3], axis=1)
        upper = pltpu.roll(jnp.concatenate(column[2:6], axis=1), 416, 1)
        down = pltpu.roll(jnp.concatenate(column[5:8] + [tail], axis=1), 448, 1)
        half = slice(HALF * q, HALF * q + HALF)
        for acc, new, value in ((ag, ng_ref, gate), (au, nu_ref, upper), (ad, nd_ref, down)):
            new[half, :] = acc[half, :] + factor * value[:, 0:UNITS]


def local(x_next, x_prev, grad_out, gate_w, up_w, down_w, acc_gate, acc_up, acc_down):
    _, ids = gather_plan()
    vmem = pl.BlockSpec(memory_space=pltpu.VMEM)
    hbm = pl.BlockSpec(memory_space=pl.ANY)
    dma = pltpu.SemaphoreType.DMA
    total_rows = x_prev.shape[0] * NZ * NY * NX * NC
    factor = 1.0 / math.sqrt(total_rows)
    rows = jax.ShapeDtypeStruct((TOKENS, 2048), BF16)
    out_next, hidden, grad_input, grads = pl.pallas_call(
        layer,
        out_shape=(
            rows, jax.ShapeDtypeStruct((GROUP, SEG), BF16), rows, jax.ShapeDtypeStruct((NC, PACK, 128), F32),
        ),
        in_specs=[hbm] * 6,
        out_specs=(hbm,) * 4,
        scratch_shapes=[
            pltpu.VMEM((3, TOKENS, 2048), BF16),
            pltpu.VMEM((3, ROWS, UNITS), BF16),
            pltpu.VMEM((NC, PACK, 128), BF16),
            pltpu.VMEM((NZ * NY, NC, PACK, 128), BF16),
            pltpu.VMEM((3 * NB, TOKENS, 2048), BF16),
            pltpu.VMEM((NZ, ZB, GROUP), BF16),
            pltpu.VMEM((NZ, ZB, GROUP), BF16),
            pltpu.VMEM((GROUP, 768), F32),
            pltpu.VMEM((GROUP, 512), F32),
            pltpu.VMEM((GROUP, 2 * SEG), F32),
            pltpu.VMEM((GROUP, 2 * SEG), BF16),
            pltpu.VMEM((GROUP, 512), BF16),
            pltpu.VMEM((GROUP, SEG), BF16),
            pltpu.VMEM((GROUP, 512), BF16),
            pltpu.VMEM((GROUP, SEG), BF16),
            pltpu.VMEM((NZ, NY, NC, PACK, 128), BF16),
            pltpu.VMEM((NZ, NY, PACK, 128), BF16),
            pltpu.VMEM((9, 5, PACK, 128), BF16),
            pltpu.VMEM((9, 5, PACK, 128), BF16),
            pltpu.VMEM((2, NC, PACK, 128), BF16),
            pltpu.VMEM((2, PACK, 128), BF16),
            pltpu.VMEM((NC, PACK, 128), F32),
            pltpu.VMEM((2, NB, TOKENS, 2048), BF16),
            pltpu.VMEM((2, 6, TOKENS, 2048), BF16),
            pltpu.VMEM((2, 2, TOKENS, 2048), BF16),
            pltpu.VMEM((2, NC, TOKENS, 2048), BF16),
            pltpu.VMEM((2, NC, TOKENS, 2048), BF16),
            pltpu.VMEM((2, TOKENS, 2048), BF16),
            dma, dma((len(ids),)), dma, dma, dma, dma((len(EZ),)), dma, dma((3, NC)), dma, dma((3, 4)),
            dma, dma((len(EZ),)), dma, dma((len(ids),)), dma, dma((2, NC)), dma, dma,
            dma, dma((2, 2, 6)), dma, dma((2, 2, 2)),
            dma, dma, dma((4,)), dma((6,)),
        ],
        compiler_params=pltpu.CompilerParams(
            collective_id=0, has_side_effects=True, vmem_limit_bytes=60 * 1024 * 1024
        ),
        name="layer",
    )(x_next, x_prev, grad_out, gate_w, up_w, down_w.T)
    sums = jax.ShapeDtypeStruct((ROWS, UNITS), F32)
    out_next, hidden, grad_input, new_gate, new_up, new_down = pl.pallas_call(
        functools.partial(finish, factor),
        out_shape=(rows, jax.ShapeDtypeStruct((GROUP, UNITS), BF16), rows, sums, sums, sums),
        in_specs=[hbm] * 7,
        out_specs=(vmem,) * 6,
        scratch_shapes=[pltpu.VMEM((GROUP, SEG), BF16), pltpu.VMEM((NC, PACK, 128), F32)]
        + [pltpu.VMEM((ROWS, UNITS), F32)] * 3 + [dma((7,))],
        compiler_params=pltpu.CompilerParams(vmem_limit_bytes=60 * 1024 * 1024),
        name="finish",
    )(out_next, hidden, grad_input, grads, acc_gate, acc_up, acc_down.T)
    return out_next, hidden, grad_input, new_gate, new_up, new_down.T


def solution(mesh):
    split = Mesh(mesh.devices.reshape(NZ, NY, NX, NC), ("z", "y", "x", "c"))
    in_specs = (
        P(TOK, None), P(TOK, None), P(TOK, None),
        P(FS, TP), P(FS, TP), P(TP, FS), P(FS, TP), P(FS, TP), P(TP, FS),
    )
    out_specs = (P(TOK, None), P(FS, TP), P(TOK, None), P(FS, TP), P(FS, TP), P(TP, FS))
    return jax.shard_map(local, mesh=split, in_specs=in_specs, out_specs=out_specs, check_vma=False)
```

```python
import functools
import heapq
import math

import jax
import jax.numpy as jnp
from jax import lax
from jax.experimental import pallas as pl
from jax.experimental.pallas import tpu as pltpu
from jax.sharding import Mesh
from jax.sharding import PartitionSpec as P

MESH = pl.DeviceIdType.MESH
F32, BF16 = jnp.float32, jnp.bfloat16
TOK = ("z", "y", "x", "c")
FS, TP = ("z", "y"), ("x", "c")
NZ, NY, NX, NC = 8, 4, 4, 2
NB = NX * NC
PACK = 264
ROWS, HALF = 64, 32
UNITS = 352
SEG = 384
ZB = NY * ROWS
TOKENS = 24
GROUP = NB * TOKENS
LATE = 5
LATENCY, ROW_US = 1.8, 1.45 / 264

EZ = (0, 1, -1, 2, -2, 3, -3, 4)
EY = (0, 1, -1, 2)
REDUCE = (
    (4, 2), (3, 2), (-3, 2), (-2, 2), (2, 2), (4, -1), (4, 1), (-1, 2), (3, -1), (3, 1), (1, 2), (-3, -1), (-3, 1),
    (4, 0), (0, 2), (-2, -1), (-2, 1), (3, 0), (2, -1), (2, 1), (-1, -1), (-1, 1), (-3, 0), (1, -1), (1, 1), (0, -1),
    (0, 1), (-2, 0), (2, 0), (-1, 0), (1, 0),
)


def rows_of(m):
    ez, ey = m
    if abs(ey) == 2:
        return (0, 128) if ey > 0 else (128, PACK)
    if ey == 0 and abs(ez) == 4:
        return (0, 128) if ez > 0 else (128, PACK)
    return 0, PACK


def sends_of(n):
    ez, ey = n
    if abs(ey) == 1:
        return [(ez, 2 * ey)]
    if ey:
        return []
    along_y = [(ez, 1), (ez, -1)]
    if abs(ez) in (1, 2):
        return along_y + [(ez + (2 if ez > 0 else -2), 0)]
    return along_y


def node_of(m):
    ez, ey = m
    return (abs(ez) if ez == -4 else ez, abs(ey) if ey == -2 else ey)


def parts_of(n):
    ez, ey = n
    if ey == 2:
        return [(ez, 2), (ez, -2)]
    return [(4, 0), (-4, 0)] if n == (4, 0) else [n]


def step_of(m):
    ez, ey = m
    if ey:
        return "y", 1 if ey > 0 else -1
    return "z", (1 if abs(ez) == 1 else 2) * (1 if ez > 0 else -1)


def widened(v, lanes):
    return jnp.concatenate([v, jnp.zeros((v.shape[0], lanes - v.shape[1]), v.dtype)], axis=1)


def known(v):
    v = v[:, 0:SEG]
    return jnp.where(lax.broadcasted_iota(jnp.int32, v.shape, 1) < UNITS, v, 0.0)


def packed_pair(gate, upper):
    both = pltpu.roll(widened(upper, 512), 96, 1)
    return jnp.concatenate([gate[:, 0:256], gate[:, 256:384] + both[:, 0:128], both[:, 128:512]], axis=1)


def packed_last(down):
    return pltpu.roll(widened(down, 512), 64, 1)


def folded(v):
    v = v.reshape(v.shape[0] // HALF, 4, 8, 128)
    total = v[:, 0].reshape(-1, 128)
    for k in range(1, 4):
        total = total + pltpu.roll(v[:, k].reshape(-1, 128), 32 * k, 1)
    return total


def unfolded(v):
    n = v.shape[0] // 8
    keep = lax.broadcasted_iota(jnp.int32, v.shape, 1) < 32
    parts = [jnp.where(keep, v if k == 0 else pltpu.roll(v, 128 - 32 * k, 1), 0.0).reshape(n, 1, 8, 128) for k in range(4)]
    return jnp.concatenate(parts, axis=1).reshape(HALF * n, 128)


@functools.lru_cache
def gather_plan():
    free, heap, got, order, ends = {}, [], set(), [], {}

    def push(now, m):
        axis, step = step_of(m)
        lo, hi = rows_of(m)
        cost = (hi - lo) * ROW_US * abs(step) if abs(m[0]) > 2 or m[1] else PACK * ROW_US * abs(step)
        link = axis, step > 0
        free[link] = max(now, free.get(link, 0.0)) + cost
        ends[m] = free[link]
        heapq.heappush(heap, (free[link] + LATENCY + 0.7 * (abs(step) - 1), len(ends), m))

    def issue(now, n):
        order.append((n, now))
        for m in sends_of(n):
            if m == (3, 0):
                push(now, (2, 0))
                push(now, (-2, 0))
            push(now, m)

    push(0.0, (1, 0))
    push(0.0, (-1, 0))
    issue(0.5, (0, 0))
    while heap:
        t, _, m = heapq.heappop(heap)
        got.add(m)
        if all(q in got for q in parts_of(node_of(m))):
            issue(t, node_of(m))
    ids = {m: i for i, m in enumerate(ends)}
    return order, ids


def layer(
    xn_in, xp_in, go_in, gw_in, uw_in, dw_in,
    out_ref, hid_ref, gin_ref, wg_out,
    mine, ours, own, w, tok, xpt, got, accp, accd, accn, gg, hp, hid, hidp, hidv, gb, gr, s, r, far_sum, home_in, home,
    part, ring, ringed, plane, crossed, outv,
    ag_s, ag_r, home_s, home_r, twin_s, twin_r, hop_s, hop_r, tk_s, tk_r,
    gift_s, gift_r, rs_s, rs_r, top_s, top_r, back_s, back_r, ring_s, ring_r, plane_s, plane_r,
    hid_s, hid_r, out_s, in_s,
):
    z, y, x, c = (lax.axis_index(a) for a in ("z", "y", "x", "c"))
    par = lax.rem(z, 2)
    zp = z + 1 - 2 * par
    j = x * NC + c
    me = z * NY + y
    keeps = c == par
    moves = c != par
    size = {"z": NZ, "y": NY, "x": NX}
    here = {"z": z, "y": y, "x": x}

    def at(axis, step):
        return lax.rem(here[axis] + (step + size[axis]), size[axis])

    barrier = pltpu.get_barrier_semaphore()
    friends = [{"z": at("z", d), "c": q} for d in (1, -1, 2, -2) for q in range(NC)]
    friends += [{"y": at("y", 1)}, {"y": at("y", -1)}, {"x": at("x", 1)}, {"x": at("x", -1)}, {"c": 1 - c}]
    for friend in friends:
        pl.semaphore_signal(barrier, inc=1, device_id=friend, device_id_type=MESH)

    loads = [(ref, ours.at[i]) for i, ref in enumerate((gw_in, uw_in, dw_in))]
    loads += [(ref, mine.at[i]) for i, ref in enumerate((xp_in, go_in, xn_in))]
    loads = [pltpu.make_async_copy(src, dst, in_s.at[i]) for i, (src, dst) in enumerate(loads)]
    for copy in loads:
        copy.start()

    for copy in loads[0:3]:
        copy.wait()

    gate_up_down = [widened(ours[i].astype(F32), SEG) for i in range(3)]
    pair = packed_pair(*gate_up_down[0:2])
    last = packed_last(gate_up_down[2])
    for q in range(NC):
        rows = slice(HALF * q, HALF * q + HALF)
        for t in range(8):
            column = jnp.zeros((HALF, 128), F32)
            if t < 6:
                column = column + pair[rows, 128 * t:128 * t + 128]
            if t > 4:
                column = column + last[rows, 128 * (t - 5):128 * (t - 4)]
            own[q, HALF * t:HALF * t + HALF, :] = column.astype(BF16)
        own[q, 256:PACK, :] = folded(last[rows, 384:512]).astype(BF16)

    for copy in loads[3:]:
        copy.wait()

    @pl.when(keeps)
    def _():
        w[me] = own[...]
        for a in range(3):
            tok[NB * a + j] = mine[a]

    with jax.named_scope("barrier"):
        pl.semaphore_wait(barrier, len(friends))

    def remote(src, dst, ssem, rsem, device):
        pltpu.make_async_remote_copy(
            src_ref=src, dst_ref=dst, send_sem=ssem, recv_sem=rsem, device_id=device, device_id_type=MESH
        ).start()

    def expect(dst, sem):
        pltpu.make_async_copy(dst, dst, sem).wait()

    order, ids = gather_plan()

    def chunk_at(n):
        return at("z", -n[0]) * NY + at("y", -n[1])

    def own_sends(step):
        for sign in (1, -1):
            for q in range(NC):
                remote(
                    own.at[q], w.at[me, q], top_s, ag_r.at[ids[(sign * step, 0)]],
                    {"z": at("z", sign * step), "c": q},
                )

    @pl.when(keeps)
    def _():
        remote(own, w.at[me], home_s, home_r, {"c": 1 - c})

    @pl.when(moves)
    def _():
        own_sends(1)

    @pl.when(moves)
    def _():
        for a in range(3):
            remote(mine.at[a], tok.at[NB * a + j], hop_s, hop_r.at[a, c], {"c": 1 - c})

    def hop(a, who):
        block = tok.at[NB * a + j]

        @pl.when(who)
        def _():
            remote(mine.at[a], block, hop_s, hop_r.at[a, c], {"z": zp, "c": par})

    hop(0, c >= 0)
    hop(1, moves)

    @pl.when(moves)
    def _():
        expect(w.at[me], home_r)

    def forward(n):
        ch = chunk_at(n)
        for m in sends_of(n):
            if m == (3, 0):

                @pl.when(keeps)
                def _():
                    own_sends(2)

                hop(1, keeps)

            lo, hi = rows_of(m)
            piece = w.at[ch, c, pl.ds(lo, hi - lo)]
            axis, step = step_of(m)
            remote(piece, piece, ag_s, ag_r.at[ids[m]], {axis: at(axis, step)})
        if n != (0, 0):
            remote(w.at[ch, c], w.at[ch, c], twin_s, twin_r.at[EZ.index(n[0])], {"c": 1 - c})

    def tok_pair(a):
        pair = tok.at[pl.ds(NB * a + x * NC, NC)]
        for i, sign in enumerate((1, -1)):
            remote(pair, pair, tk_s, tk_r.at[a, i], {"x": at("x", sign)})

    def tok_stay(a):
        @pl.when(keeps)
        def _():
            expect(tok.at[NB * a + x * NC + 1 - c], hop_r.at[a, 1 - c])
            tok_pair(a)

    def tok_hop(a):
        @pl.when(moves)
        def _():
            for q in range(NC):
                expect(tok.at[NB * a + x * NC + q], hop_r.at[a, q])
            tok_pair(a)

    def tok_near(a, who):
        @pl.when(who)
        def _():
            for i, sign in enumerate((1, -1)):
                first = NB * a + at("x", -sign) * NC
                expect(tok.at[pl.ds(first, NC)], tk_r.at[a, i])
                block = tok.at[first + i]
                remote(block, block, tk_s, tk_r.at[a, 2 + i], {"x": at("x", sign)})

    def tok_far(a):
        for i in range(2):
            expect(tok.at[NB * a + at("x", 2) * NC + i], tk_r.at[a, 2 + i])

    def cols(zb):
        return pl.ds(pl.multiple_of(zb * ZB, ZB), ZB)

    def weights(zb, first, end):
        parts = [w[pl.ds(zb * NY, NY), :, HALF * t:HALF * t + HALF, :].reshape(ZB, 128) for t in range(first, min(end, 8))]
        if end > 8:
            tail = w[pl.ds(zb * NY, NY), :, 256:PACK, :].astype(F32).reshape(NY * NC * 8, 128)
            parts.append(unfolded(tail).astype(BF16))
        return jnp.concatenate(parts, axis=1)

    eye_zb = (
        lax.broadcasted_iota(jnp.int32, (ZB, ZB), 0) == lax.broadcasted_iota(jnp.int32, (ZB, ZB), 1)
    ).astype(BF16)

    def turn(a, dst, zb):
        block = tok[NB * a:NB * a + NB, :, cols(zb)].reshape(GROUP, ZB)
        dst[zb] = lax.dot_general(
            eye_zb, block, (((1,), (1,)), ((), ())), preferred_element_type=F32
        ).astype(BF16)

    def project(a, acc, columns, zb, first):
        block = tok[NB * a:NB * a + NB, :, cols(zb)].reshape(GROUP, ZB)
        value = jnp.dot(block, weights(zb, *columns), preferred_element_type=F32)
        if first:
            acc[...] = value
        else:
            acc[...] += value

    def block_steps(e):
        return (e,) if e in (0, 4) else (e, -e)

    done = set()
    turns = [functools.partial(turn, a, dst, at("z", -ez)) for a, dst in ((0, xpt), (1, got)) for ez in EZ[NZ - LATE:]]

    def project_block(a, e):
        for ez in block_steps(e):
            if ez not in twins:
                count = NY - 1 if ez == 0 else NY
                expect(w.at[pl.ds(0, count), 1 - c], twin_r.at[EZ.index(ez)])
                twins.add(ez)
            project(a, (accp, accd)[a], ((0, 6), (5, 9))[a], at("z", -ez), ez == 0)
        done.add((a, e))

    twins, ready = set(), set()

    def fill(i):
        for a in range(2):
            for e in range(5):
                if a in ready and (a, e) not in done and i > last_of[e]:
                    project_block(a, e)
                    break
        for _ in range(2):
            if turns and (1 if len(turns) <= LATE else 0) in ready:
                turns.pop(0)()

    last_of = {
        e: max(i for i, (n, _) in enumerate(order) if abs(n[0]) == e) for e in range(5)
    }

    def tok_last(a):
        tok_far(a)
        ready.add(a)

    timed = [
        (1.0, tok_stay, 0), (1.1, tok_stay, 1), (6.4, tok_near, 0, keeps), (6.6, tok_hop, 0), (9.0, tok_near, 1, keeps),
        (9.1, hop, 2, c >= 0), (10.9, tok_hop, 1), (11.0, tok_near, 0, moves), (15.0, tok_near, 1, moves), (15.1, tok_stay, 2),
        (15.2, tok_hop, 2), (16.0, tok_last, 0), (19.7, tok_last, 1), (22.5, tok_near, 2, c >= 0),
    ]
    for i, (n, t) in enumerate(order):
        while timed and timed[0][0] <= (t if i + 1 < len(order) else 99):
            when, work, *given = timed.pop(0)
            with jax.named_scope("t#%s%.1f" % (work.__name__, when)):
                work(*given)
        with jax.named_scope("ga#i=%d#z=%d#y=%d" % (i, *n)):
            if n != (0, 0):
                for m in parts_of(n):
                    lo, hi = rows_of(m)
                    expect(w.at[chunk_at(n), c, pl.ds(lo, hi - lo)], ag_r.at[ids[m]])
            forward(n)
        if ready:
            with jax.named_scope("fill#i=%d" % i):
                fill(i)
    for work in turns:
        work()
    for e in range(5):
        for a in range(2):
            if (a, e) not in done:
                project_block(a, e)

    gate = known(accp[...])
    upper = known(pltpu.roll(accp[...], 768 - UNITS, 1))
    grad_h = known(pltpu.roll(accd[...], 448, 1))
    sig = 1.0 / (1.0 + jnp.exp(-gate))
    silu = gate * sig
    gg[...] = packed_pair(
        grad_h * upper * sig * (1.0 + gate * (1.0 - sig)), grad_h * silu
    ).astype(BF16)
    hp[...] = packed_last(silu * upper).astype(BF16)

    def weight_grad(ez):
        zb = at("z", -ez)
        if ez in EZ[:NZ - LATE]:
            turn(0, xpt, zb)
            turn(1, got, zb)
        pair = jnp.dot(xpt[zb], gg[...], preferred_element_type=F32)
        last = jnp.dot(got[zb], hp[...], preferred_element_type=F32)
        for t in range(8):
            if t < 5:
                column = pair[:, 128 * t:128 * t + 128]
            elif t == 5:
                column = pair[:, 640:768] + last[:, 0:128]
            else:
                column = last[:, 128 * (t - 5):128 * (t - 4)]
            gb[zb, :, :, HALF * t:HALF * t + HALF, :] = column.astype(BF16).reshape(NY, NC, HALF, 128)
        gb[zb, :, :, 256:PACK, :] = folded(last[:, 384:512]).astype(BF16).reshape(NY, NC, 8, 128)
        remote(gb.at[zb, :, 1 - c], gr.at[zb], gift_s, gift_r.at[EZ.index(ez)], {"c": 1 - c})

    gifted = set()

    def add_up(n, store):
        ez, _ = n
        if ez not in gifted:
            expect(gr.at[at("z", -ez)], gift_r.at[EZ.index(ez)])
            gifted.add(ez)
        kids = [(m, rows_of(m)) for m in sends_of(n)]
        for m, (a, b) in kids:
            expect(r.at[m[0] + 4, m[1] + 2, pl.ds(a, b - a)], rs_r.at[ids[m]])
        edges = sorted({0, PACK, *(v for _, ab in kids for v in ab)})
        zb, yb = at("z", -ez), at("y", -n[1])
        for a, b in zip(edges, edges[1:]):
            total = gb[zb, yb, c, a:b, :].astype(F32) + gr[zb, yb, a:b, :].astype(F32)
            for m, (ka, kb) in kids:
                if ka <= a and b <= kb:
                    total = total + r[m[0] + 4, m[1] + 2, a:b, :].astype(F32)
            store(a, b, total)

    def give(n):
        sz, sy = n[0] + 4, n[1] + 2

        def store(a, b, total):
            s[sz, sy, a:b, :] = total.astype(BF16)

        add_up(n, store)
        for m in parts_of(n):
            a, b = rows_of(m)
            axis, step = step_of(m)
            piece = s.at[sz, sy, pl.ds(a, b - a)]
            if m[1] == 0 and abs(m[0]) <= 2:
                side = 0 if m[0] > 0 else 1
                remote(piece, far_sum.at[side, c], back_s, top_r.at[side, c], {"z": at("z", -step), "c": par})
            else:
                remote(
                    piece, r.at[m[0] + 4, m[1] + 2, pl.ds(a, b - a)], rs_s, rs_r.at[ids[m]],
                    {axis: at(axis, -step)},
                )

    outs = []

    def share(which, left, columns, zb):
        value = lax.dot_general(
            left[...], weights(zb, *columns),
            (((1,), (1,)), ((), ())), preferred_element_type=F32,
        ).astype(BF16).reshape(NB, TOKENS, ZB)
        part[which, :, :, ZB * zb:ZB * zb + ZB] = value
        if zb % 4 == 3:
            h = zb // 4
            over, under, across = at("x", 1), at("x", -1), at("x", 2)
            for i, (block, to) in enumerate((
                (across * NC, over), (over * NC + 1, over), (across * NC + 1, under), (under * NC, under),
            )):
                remote(
                    part.at[which, block, :, wide[h]], ring.at[which, i, :, wide[h]],
                    ring_s, ring_r.at[which, h, i], {"x": to},
                )

    wide = (pl.ds(0, 1024), pl.ds(1024, 1024))

    def share_on(which, h):
        for i, (at_ring, sign) in enumerate(((0, 1), (2, -1))):
            to = at("x", sign)
            expect(ring.at[which, at_ring, :, wide[h]], ring_r.at[which, h, at_ring])
            ringed[which, i, :, wide[h]] = (
                part[which, to * NC + i, :, wide[h]].astype(F32) + ring[which, at_ring, :, wide[h]].astype(F32)
            ).astype(BF16)
            remote(
                ringed.at[which, i, :, wide[h]], ring.at[which, 4 + i, :, wide[h]],
                ring_s, ring_r.at[which, h, 4 + i], {"x": to},
            )

    def share_plane(which, h):
        for i in (1, 3, 4, 5):
            expect(ring.at[which, i, :, wide[h]], ring_r.at[which, h, i])
        for q, (i, k) in enumerate(((3, 4), (1, 5))):
            plane[which, q, :, wide[h]] = (
                part[which, x * NC + q, :, wide[h]].astype(F32)
                + ring[which, i, :, wide[h]].astype(F32) + ring[which, k, :, wide[h]].astype(F32)
            ).astype(BF16)

        @pl.when(moves)
        def _():
            for q in range(NC):
                remote(
                    plane.at[which, q, :, wide[h]], crossed.at[which, 0, :, wide[h]],
                    plane_s, plane_r.at[which, h, 0], {"z": zp, "c": q},
                )

        @pl.when(keeps)
        def _():
            remote(
                plane.at[which, 1 - c, :, wide[h]], crossed.at[which, 1, :, wide[h]],
                plane_s, plane_r.at[which, h, 1], {"c": 1 - c},
            )

    def put(src, dst, i):
        pltpu.make_async_copy(src, dst, out_s.at[i]).start()

    def share_final(which, out):
        for h in range(2):
            expect(crossed.at[which, 0, :, wide[h]], plane_r.at[which, h, 0])

        @pl.when(keeps)
        def _():
            outv[which] = (plane[which, c].astype(F32) + crossed[which, 0].astype(F32)).astype(BF16)

        @pl.when(moves)
        def _():
            for h in range(2):
                expect(crossed.at[which, 1, :, wide[h]], plane_r.at[which, h, 1])
            outv[which] = (crossed[which, 1].astype(F32) + crossed[which, 0].astype(F32)).astype(BF16)

        put(outv.at[which], out, which)

    def forward_gate():
        gate = known(accn[...])
        upper = known(pltpu.roll(accn[...], 768 - UNITS, 1))
        value = gate * (1.0 / (1.0 + jnp.exp(-gate))) * upper
        hid[...] = value.astype(BF16)
        hidp[...] = packed_last(value).astype(BF16)

        @pl.when(keeps)
        def _():
            put(hid, hid_ref, 2)

        @pl.when(moves)
        def _():
            remote(hid, hidv, hid_s, hid_r, {"z": zp, "c": 1 - c})

    def hidden_out():
        @pl.when(moves)
        def _():
            expect(hidv, hid_r)
            put(hidv, hid_ref, 2)

    def next_blocks(ezs):
        for ez in ezs:
            project(2, accn, (0, 6), at("z", -ez), ez == 0)

    def share_in(zb):
        share(1, gg, (0, 6), zb)

    def share_next(zb):
        share(0, hidp, (5, 9), zb)

    plan = [(0, share_in, 0)] + [(3 + (i - 1) // 2, share_in, i) for i in range(1, NZ)]
    plan += [(7, tok_far, 2), (7, next_blocks, EZ[0:4]), (8, next_blocks, EZ[4:8]), (9, forward_gate)]
    plan += [(9, share_next, 0), (9, share_on, 1, 0), (10, share_next, 1), (10, share_next, 2), (11, share_next, 3)]
    plan += [(11, share_next, 4), (12, share_next, 5), (12, share_on, 1, 1), (13, share_next, 6), (13, share_next, 7)]
    plan += [
        (20, share_plane, 1, 0), (22, share_on, 0, 0), (25, share_plane, 1, 1), (29, share_on, 0, 1),
        (29, hidden_out), (29, share_plane, 0, 0), (31, share_plane, 0, 1),
        (92, share_final, 1, gin_ref), (93, share_final, 0, out_ref),
    ]

    def between(until):
        while plan and plan[0][0] <= until:
            _, work, *given = plan.pop(0)
            with jax.named_scope("w#%s" % "_".join([work.__name__] + [str(v) for v in given if isinstance(v, int)])):
                work(*given)

    graded = set()
    for count, n in enumerate(REDUCE):
        for e in (abs(n[0]), abs(n[0]) - 1):
            if e >= 0 and e not in graded:
                with jax.named_scope("wgrad#e=%d" % e):
                    for ez in block_steps(e):
                        weight_grad(ez)
                graded.add(e)
        between(count)
        with jax.named_scope("give#i=%d#z=%d#y=%d" % (count, *n)):
            give(n)
        between(count + 1)

    with jax.named_scope("last"):

        @pl.when(moves)
        def _():
            home[...] = jnp.zeros((NC, PACK, 128), F32)

        def keep(a, b, total):
            home_in[0, a:b, :] = total.astype(BF16)

            @pl.when(keeps)
            def _():
                home[c, a:b, :] = total

        add_up((0, 0), keep)

        @pl.when(moves)
        def _():
            remote(home_in.at[0], home_in.at[1], home_s, home_r, {"c": 1 - c})

    between(99)
    with jax.named_scope("final"):

        @pl.when(keeps)
        def _():
            expect(home_in.at[1], home_r)
            home[1 - c] = home_in[1].astype(F32)

        for side in range(2):
            for q in range(NC):
                expect(far_sum.at[side, q], top_r.at[side, q])
        for q in range(NC):
            home[q] = (
                home[q] + far_sum[0, q].astype(F32) + far_sum[1, q].astype(F32)
            )
        put(home, wg_out, 3)
    with jax.named_scope("drain"):
        routed = sum(rows_of(m)[1] - rows_of(m)[0] for m in ids if m[1] or abs(m[0]) > 2) // PACK
        for count, sem in ((routed, ag_s), (routed, rs_s), (4, top_s), (4, back_s), (NZ * NY - 1, twin_s)):
            expect(w.at[pl.ds(0, count), 0], sem)
        expect(gr, gift_s)
        for count, sem in ((18, tk_s), (12, ring_s)):
            expect(tok.at[pl.ds(0, count)], sem)

        @pl.when(keeps)
        def _():
            expect(own, home_s)
            expect(tok.at[pl.ds(0, 3)], hop_s)
            expect(tok.at[pl.ds(0, 2)], plane_s)

        @pl.when(moves)
        def _():
            expect(home_in.at[0], home_s)
            expect(tok.at[pl.ds(0, 6)], hop_s)
            expect(tok.at[pl.ds(0, 4)], plane_s)
            expect(hid, hid_s)

        for i, (src, dst) in enumerate(((outv.at[0], out_ref), (outv.at[1], gin_ref), (hid, hid_ref), (home, wg_out))):
            pltpu.make_async_copy(src, dst, out_s.at[i]).wait()


def finish(
    factor, out_in, hid_in, gin_in, wg_in, ag_in, au_in, ad_in,
    out_ref, hid_ref, gin_ref, ng_ref, nu_ref, nd_ref, hidv, wg, ag, au, ad, sems,
):
    pairs = ((wg_in, wg), (out_in, out_ref), (gin_in, gin_ref), (hid_in, hidv), (ag_in, ag), (au_in, au), (ad_in, ad))
    copies = [pltpu.make_async_copy(src, dst, sems.at[i]) for i, (src, dst) in enumerate(pairs)]
    for copy in copies:
        copy.start()
    for copy in copies:
        copy.wait()
    hid_ref[...] = hidv[:, 0:UNITS]
    for q in range(NC):
        column = [wg[q, HALF * t:HALF * t + HALF, :] for t in range(8)]
        tail = unfolded(wg[q, 256:PACK, :])
        gate = jnp.concatenate(column[0:3], axis=1)
        upper = pltpu.roll(jnp.concatenate(column[2:6], axis=1), 416, 1)
        down = pltpu.roll(jnp.concatenate(column[5:8] + [tail], axis=1), 448, 1)
        half = slice(HALF * q, HALF * q + HALF)
        for acc, new, value in ((ag, ng_ref, gate), (au, nu_ref, upper), (ad, nd_ref, down)):
            new[half, :] = acc[half, :] + factor * value[:, 0:UNITS]


def local(x_next, x_prev, grad_out, gate_w, up_w, down_w, acc_gate, acc_up, acc_down):
    _, ids = gather_plan()
    vmem = pl.BlockSpec(memory_space=pltpu.VMEM)
    hbm = pl.BlockSpec(memory_space=pl.ANY)
    dma = pltpu.SemaphoreType.DMA
    total_rows = x_prev.shape[0] * NZ * NY * NX * NC
    factor = 1.0 / math.sqrt(total_rows)
    rows = jax.ShapeDtypeStruct((TOKENS, 2048), BF16)
    out_next, hidden, grad_input, grads = pl.pallas_call(
        layer,
        out_shape=(
            rows, jax.ShapeDtypeStruct((GROUP, SEG), BF16), rows, jax.ShapeDtypeStruct((NC, PACK, 128), F32),
        ),
        in_specs=[hbm] * 6,
        out_specs=(hbm,) * 4,
        scratch_shapes=[
            pltpu.VMEM((3, TOKENS, 2048), BF16),
            pltpu.VMEM((3, ROWS, UNITS), BF16),
            pltpu.VMEM((NC, PACK, 128), BF16),
            pltpu.VMEM((NZ * NY, NC, PACK, 128), BF16),
            pltpu.VMEM((3 * NB, TOKENS, 2048), BF16),
            pltpu.VMEM((NZ, ZB, GROUP), BF16),
            pltpu.VMEM((NZ, ZB, GROUP), BF16),
            pltpu.VMEM((GROUP, 768), F32),
            pltpu.VMEM((GROUP, 512), F32),
            pltpu.VMEM((GROUP, 2 * SEG), F32),
            pltpu.VMEM((GROUP, 2 * SEG), BF16),
            pltpu.VMEM((GROUP, 512), BF16),
            pltpu.VMEM((GROUP, SEG), BF16),
            pltpu.VMEM((GROUP, 512), BF16),
            pltpu.VMEM((GROUP, SEG), BF16),
            pltpu.VMEM((NZ, NY, NC, PACK, 128), BF16),
            pltpu.VMEM((NZ, NY, PACK, 128), BF16),
            pltpu.VMEM((9, 5, PACK, 128), BF16),
            pltpu.VMEM((9, 5, PACK, 128), BF16),
            pltpu.VMEM((2, NC, PACK, 128), BF16),
            pltpu.VMEM((2, PACK, 128), BF16),
            pltpu.VMEM((NC, PACK, 128), F32),
            pltpu.VMEM((2, NB, TOKENS, 2048), BF16),
            pltpu.VMEM((2, 6, TOKENS, 2048), BF16),
            pltpu.VMEM((2, 2, TOKENS, 2048), BF16),
            pltpu.VMEM((2, NC, TOKENS, 2048), BF16),
            pltpu.VMEM((2, NC, TOKENS, 2048), BF16),
            pltpu.VMEM((2, TOKENS, 2048), BF16),
            dma, dma((len(ids),)), dma, dma, dma, dma((len(EZ),)), dma, dma((3, NC)), dma, dma((3, 4)),
            dma, dma((len(EZ),)), dma, dma((len(ids),)), dma, dma((2, NC)), dma, dma,
            dma, dma((2, 2, 6)), dma, dma((2, 2, 2)),
            dma, dma, dma((4,)), dma((6,)),
        ],
        compiler_params=pltpu.CompilerParams(
            collective_id=0, has_side_effects=True, vmem_limit_bytes=60 * 1024 * 1024
        ),
        name="layer",
    )(x_next, x_prev, grad_out, gate_w, up_w, down_w.T)
    sums = jax.ShapeDtypeStruct((ROWS, UNITS), F32)
    out_next, hidden, grad_input, new_gate, new_up, new_down = pl.pallas_call(
        functools.partial(finish, factor),
        out_shape=(rows, jax.ShapeDtypeStruct((GROUP, UNITS), BF16), rows, sums, sums, sums),
        in_specs=[hbm] * 7,
        out_specs=(vmem,) * 6,
        scratch_shapes=[pltpu.VMEM((GROUP, SEG), BF16), pltpu.VMEM((NC, PACK, 128), F32)]
        + [pltpu.VMEM((ROWS, UNITS), F32)] * 3 + [dma((7,))],
        compiler_params=pltpu.CompilerParams(vmem_limit_bytes=60 * 1024 * 1024),
        name="finish",
    )(out_next, hidden, grad_input, grads, acc_gate, acc_up, acc_down.T)
    return out_next, hidden, grad_input, new_gate, new_up, new_down.T


def solution(mesh):
    split = Mesh(mesh.devices.reshape(NZ, NY, NX, NC), ("z", "y", "x", "c"))
    in_specs = (
        P(TOK, None), P(TOK, None), P(TOK, None),
        P(FS, TP), P(FS, TP), P(TP, FS), P(FS, TP), P(FS, TP), P(TP, FS),
    )
    out_specs = (P(TOK, None), P(FS, TP), P(TOK, None), P(FS, TP), P(FS, TP), P(TP, FS))
    return jax.shard_map(local, mesh=split, in_specs=in_specs, out_specs=out_specs, check_vma=False)
```

```python
import functools
import heapq
import math

import jax
import jax.numpy as jnp
from jax import lax
from jax.experimental import pallas as pl
from jax.experimental.pallas import tpu as pltpu
from jax.sharding import Mesh
from jax.sharding import PartitionSpec as P

MESH = pl.DeviceIdType.MESH
F32, BF16 = jnp.float32, jnp.bfloat16
TOK = ("z", "y", "x", "c")
FS, TP = ("z", "y"), ("x", "c")
NZ, NY, NX, NC = 8, 4, 4, 2
NB = NX * NC
PACK = 264
ROWS, HALF = 64, 32
UNITS = 352
SEG = 384
ZB = NY * ROWS
TOKENS = 24
GROUP = NB * TOKENS
LATE = 5
LATENCY, ROW_US = 1.8, 1.45 / 264

EZ = (0, 1, -1, 2, -2, 3, -3, 4)
EY = (0, 1, -1, 2)
REDUCE = (
    (4, 2), (3, 2), (-3, 2), (-2, 2), (2, 2), (4, -1), (4, 1), (-1, 2), (3, -1), (3, 1), (1, 2), (-3, -1), (-3, 1),
    (4, 0), (0, 2), (-2, -1), (-2, 1), (3, 0), (2, -1), (2, 1), (-1, -1), (-1, 1), (-3, 0), (1, -1), (1, 1), (0, -1),
    (0, 1), (-2, 0), (2, 0), (-1, 0), (1, 0),
)


def rows_of(m):
    ez, ey = m
    if abs(ey) == 2:
        return (0, 128) if ey > 0 else (128, PACK)
    if ey == 0 and abs(ez) == 4:
        return (0, 128) if ez > 0 else (128, PACK)
    return 0, PACK


def sends_of(n):
    ez, ey = n
    if abs(ey) == 1:
        return [(ez, 2 * ey)]
    if ey:
        return []
    along_y = [(ez, 1), (ez, -1)]
    if abs(ez) in (1, 2):
        return along_y + [(ez + (2 if ez > 0 else -2), 0)]
    return along_y


def node_of(m):
    ez, ey = m
    return (abs(ez) if ez == -4 else ez, abs(ey) if ey == -2 else ey)


def parts_of(n):
    ez, ey = n
    if ey == 2:
        return [(ez, 2), (ez, -2)]
    return [(4, 0), (-4, 0)] if n == (4, 0) else [n]


def step_of(m):
    ez, ey = m
    if ey:
        return "y", 1 if ey > 0 else -1
    return "z", (1 if abs(ez) == 1 else 2) * (1 if ez > 0 else -1)


def widened(v, lanes):
    return jnp.concatenate([v, jnp.zeros((v.shape[0], lanes - v.shape[1]), v.dtype)], axis=1)


def known(v):
    v = v[:, 0:SEG]
    return jnp.where(lax.broadcasted_iota(jnp.int32, v.shape, 1) < UNITS, v, 0.0)


def packed_pair(gate, upper):
    both = pltpu.roll(widened(upper, 512), 96, 1)
    return jnp.concatenate([gate[:, 0:256], gate[:, 256:384] + both[:, 0:128], both[:, 128:512]], axis=1)


def packed_last(down):
    return pltpu.roll(widened(down, 512), 64, 1)


def folded(v):
    v = v.reshape(v.shape[0] // HALF, 4, 8, 128)
    total = v[:, 0].reshape(-1, 128)
    for k in range(1, 4):
        total = total + pltpu.roll(v[:, k].reshape(-1, 128), 32 * k, 1)
    return total


def unfolded(v):
    n = v.shape[0] // 8
    keep = lax.broadcasted_iota(jnp.int32, v.shape, 1) < 32
    parts = [jnp.where(keep, v if k == 0 else pltpu.roll(v, 128 - 32 * k, 1), 0.0).reshape(n, 1, 8, 128) for k in range(4)]
    return jnp.concatenate(parts, axis=1).reshape(HALF * n, 128)


@functools.lru_cache
def gather_plan():
    free, heap, got, order, ends = {}, [], set(), [], {}

    def push(now, m):
        axis, step = step_of(m)
        lo, hi = rows_of(m)
        cost = (hi - lo) * ROW_US * abs(step) if abs(m[0]) > 2 or m[1] else PACK * ROW_US * abs(step)
        link = axis, step > 0
        free[link] = max(now, free.get(link, 0.0)) + cost
        ends[m] = free[link]
        heapq.heappush(heap, (free[link] + LATENCY + 0.7 * (abs(step) - 1), len(ends), m))

    def issue(now, n):
        order.append((n, now))
        for m in sends_of(n):
            if m == (3, 0):
                push(now, (2, 0))
                push(now, (-2, 0))
            push(now, m)

    push(0.0, (1, 0))
    push(0.0, (-1, 0))
    issue(0.5, (0, 0))
    while heap:
        t, _, m = heapq.heappop(heap)
        got.add(m)
        if all(q in got for q in parts_of(node_of(m))):
            issue(t, node_of(m))
    ids = {m: i for i, m in enumerate(ends)}
    return order, ids


def layer(
    xn_in, xp_in, go_in, gw_in, uw_in, dw_in,
    out_ref, hid_ref, gin_ref, wg_out,
    mine, ours, own, w, tok, xpt, got, accp, accd, accn, gg, hp, hid, hidp, hidv, gb, gr, s, r, far_sum, home_in, home,
    part, ring, ringed, plane, crossed, outv,
    ag_s, ag_r, home_s, home_r, twin_s, twin_r, hop_s, hop_r, tk_s, tk_r,
    gift_s, gift_r, rs_s, rs_r, top_s, top_r, back_s, back_r, ring_s, ring_r, plane_s, plane_r,
    hid_s, hid_r, out_s, in_s,
):
    z, y, x, c = (lax.axis_index(a) for a in ("z", "y", "x", "c"))
    par = lax.rem(z, 2)
    zp = z + 1 - 2 * par
    j = x * NC + c
    me = z * NY + y
    keeps = c == par
    moves = c != par
    size = {"z": NZ, "y": NY, "x": NX}
    here = {"z": z, "y": y, "x": x}

    def at(axis, step):
        return lax.rem(here[axis] + (step + size[axis]), size[axis])

    barrier = pltpu.get_barrier_semaphore()
    friends = [{"z": at("z", d), "c": q} for d in (1, -1, 2, -2) for q in range(NC)]
    friends += [{"y": at("y", 1)}, {"y": at("y", -1)}, {"x": at("x", 1)}, {"x": at("x", -1)}, {"c": 1 - c}]
    for friend in friends:
        pl.semaphore_signal(barrier, inc=1, device_id=friend, device_id_type=MESH)

    loads = [(ref, ours.at[i]) for i, ref in enumerate((gw_in, uw_in, dw_in))]
    loads += [(ref, mine.at[i]) for i, ref in enumerate((xp_in, go_in, xn_in))]
    loads = [pltpu.make_async_copy(src, dst, in_s.at[i]) for i, (src, dst) in enumerate(loads)]
    for copy in loads:
        copy.start()

    for copy in loads[0:3]:
        copy.wait()

    gate_up_down = [widened(ours[i].astype(F32), SEG) for i in range(3)]
    pair = packed_pair(*gate_up_down[0:2])
    last = packed_last(gate_up_down[2])
    for q in range(NC):
        rows = slice(HALF * q, HALF * q + HALF)
        for t in range(8):
            column = jnp.zeros((HALF, 128), F32)
            if t < 6:
                column = column + pair[rows, 128 * t:128 * t + 128]
            if t > 4:
                column = column + last[rows, 128 * (t - 5):128 * (t - 4)]
            own[q, HALF * t:HALF * t + HALF, :] = column.astype(BF16)
        own[q, 256:PACK, :] = folded(last[rows, 384:512]).astype(BF16)

    for copy in loads[3:]:
        copy.wait()

    @pl.when(keeps)
    def _():
        w[me] = own[...]
        for a in range(3):
            tok[NB * a + j] = mine[a]

    with jax.named_scope("barrier"):
        pl.semaphore_wait(barrier, len(friends))

    def remote(src, dst, ssem, rsem, device):
        pltpu.make_async_remote_copy(
            src_ref=src, dst_ref=dst, send_sem=ssem, recv_sem=rsem, device_id=device, device_id_type=MESH
        ).start()

    def expect(dst, sem):
        pltpu.make_async_copy(dst, dst, sem).wait()

    order, ids = gather_plan()

    def chunk_at(n):
        return at("z", -n[0]) * NY + at("y", -n[1])

    def own_sends(step):
        for sign in (1, -1):
            for q in range(NC):
                remote(
                    own.at[q], w.at[me, q], top_s, ag_r.at[ids[(sign * step, 0)]],
                    {"z": at("z", sign * step), "c": q},
                )

    @pl.when(keeps)
    def _():
        remote(own, w.at[me], home_s, home_r, {"c": 1 - c})

    @pl.when(moves)
    def _():
        own_sends(1)

    @pl.when(moves)
    def _():
        for a in range(3):
            remote(mine.at[a], tok.at[NB * a + j], hop_s, hop_r.at[a, c], {"c": 1 - c})

    def hop(a, who):
        block = tok.at[NB * a + j]

        @pl.when(who)
        def _():
            remote(mine.at[a], block, hop_s, hop_r.at[a, c], {"z": zp, "c": par})

    hop(0, c >= 0)
    hop(1, moves)

    @pl.when(moves)
    def _():
        expect(w.at[me], home_r)

    def forward(n):
        ch = chunk_at(n)
        for m in sends_of(n):
            if m == (3, 0):

                @pl.when(keeps)
                def _():
                    own_sends(2)

                hop(1, keeps)

            lo, hi = rows_of(m)
            piece = w.at[ch, c, pl.ds(lo, hi - lo)]
            axis, step = step_of(m)
            remote(piece, piece, ag_s, ag_r.at[ids[m]], {axis: at(axis, step)})
        if n != (0, 0):
            remote(w.at[ch, c], w.at[ch, c], twin_s, twin_r.at[EZ.index(n[0])], {"c": 1 - c})

    def tok_pair(a):
        pair = tok.at[pl.ds(NB * a + x * NC, NC)]
        for i, sign in enumerate((1, -1)):
            remote(pair, pair, tk_s, tk_r.at[a, i], {"x": at("x", sign)})

    def tok_stay(a):
        @pl.when(keeps)
        def _():
            expect(tok.at[NB * a + x * NC + 1 - c], hop_r.at[a, 1 - c])
            tok_pair(a)

    def tok_hop(a):
        @pl.when(moves)
        def _():
            for q in range(NC):
                expect(tok.at[NB * a + x * NC + q], hop_r.at[a, q])
            tok_pair(a)

    def tok_near(a, who):
        @pl.when(who)
        def _():
            for i, sign in enumerate((1, -1)):
                first = NB * a + at("x", -sign) * NC
                expect(tok.at[pl.ds(first, NC)], tk_r.at[a, i])
                block = tok.at[first + i]
                remote(block, block, tk_s, tk_r.at[a, 2 + i], {"x": at("x", sign)})

    def tok_far(a):
        for i in range(2):
            expect(tok.at[NB * a + at("x", 2) * NC + i], tk_r.at[a, 2 + i])

    def cols(zb):
        return pl.ds(pl.multiple_of(zb * ZB, ZB), ZB)

    def weights(zb, first, end):
        parts = [w[pl.ds(zb * NY, NY), :, HALF * t:HALF * t + HALF, :].reshape(ZB, 128) for t in range(first, min(end, 8))]
        if end > 8:
            tail = w[pl.ds(zb * NY, NY), :, 256:PACK, :].astype(F32).reshape(NY * NC * 8, 128)
            parts.append(unfolded(tail).astype(BF16))
        return jnp.concatenate(parts, axis=1)

    eye_zb = (
        lax.broadcasted_iota(jnp.int32, (ZB, ZB), 0) == lax.broadcasted_iota(jnp.int32, (ZB, ZB), 1)
    ).astype(BF16)

    def turn(a, dst, zb):
        block = tok[NB * a:NB * a + NB, :, cols(zb)].reshape(GROUP, ZB)
        dst[zb] = lax.dot_general(
            eye_zb, block, (((1,), (1,)), ((), ())), preferred_element_type=F32
        ).astype(BF16)

    def project(a, acc, columns, zb, first):
        block = tok[NB * a:NB * a + NB, :, cols(zb)].reshape(GROUP, ZB)
        value = jnp.dot(block, weights(zb, *columns), preferred_element_type=F32)
        if first:
            acc[...] = value
        else:
            acc[...] += value

    def block_steps(e):
        return (e,) if e in (0, 4) else (e, -e)

    done = set()
    turns = [functools.partial(turn, a, dst, at("z", -ez)) for a, dst in ((0, xpt), (1, got)) for ez in EZ[NZ - LATE:]]

    def project_block(a, e):
        for ez in block_steps(e):
            if ez not in twins:
                count = NY - 1 if ez == 0 else NY
                expect(w.at[pl.ds(0, count), 1 - c], twin_r.at[EZ.index(ez)])
                twins.add(ez)
            project(a, (accp, accd)[a], ((0, 6), (5, 9))[a], at("z", -ez), ez == 0)
        done.add((a, e))

    twins, ready = set(), set()

    def fill(i):
        for a in range(2):
            for e in range(5):
                if a in ready and (a, e) not in done and i > last_of[e]:
                    project_block(a, e)
                    break
        for _ in range(2):
            if turns and (1 if len(turns) <= LATE else 0) in ready:
                turns.pop(0)()

    last_of = {
        e: max(i for i, (n, _) in enumerate(order) if abs(n[0]) == e) for e in range(5)
    }

    def tok_last(a):
        tok_far(a)
        ready.add(a)

    timed = [
        (1.0, tok_stay, 0), (1.1, tok_stay, 1), (6.4, tok_near, 0, keeps), (6.6, tok_hop, 0), (9.0, tok_near, 1, keeps),
        (10.9, tok_hop, 1), (11.0, tok_near, 0, moves), (12.3, hop, 2, c >= 0), (15.0, tok_near, 1, moves), (15.1, tok_stay, 2),
        (15.2, tok_hop, 2), (16.0, tok_last, 0), (19.7, tok_last, 1), (22.5, tok_near, 2, c >= 0),
    ]
    for i, (n, t) in enumerate(order):
        while timed and timed[0][0] <= (t if i + 1 < len(order) else 99):
            when, work, *given = timed.pop(0)
            with jax.named_scope("t#%s%.1f" % (work.__name__, when)):
                work(*given)
        with jax.named_scope("ga#i=%d#z=%d#y=%d" % (i, *n)):
            if n != (0, 0):
                for m in parts_of(n):
                    lo, hi = rows_of(m)
                    expect(w.at[chunk_at(n), c, pl.ds(lo, hi - lo)], ag_r.at[ids[m]])
            forward(n)
        if ready:
            with jax.named_scope("fill#i=%d" % i):
                fill(i)
    for work in turns:
        work()
    for e in range(5):
        for a in range(2):
            if (a, e) not in done:
                project_block(a, e)

    gate = known(accp[...])
    upper = known(pltpu.roll(accp[...], 768 - UNITS, 1))
    grad_h = known(pltpu.roll(accd[...], 448, 1))
    sig = 1.0 / (1.0 + jnp.exp(-gate))
    silu = gate * sig
    gg[...] = packed_pair(
        grad_h * upper * sig * (1.0 + gate * (1.0 - sig)), grad_h * silu
    ).astype(BF16)
    hp[...] = packed_last(silu * upper).astype(BF16)

    def weight_grad(ez):
        zb = at("z", -ez)
        if ez in EZ[:NZ - LATE]:
            turn(0, xpt, zb)
            turn(1, got, zb)
        pair = jnp.dot(xpt[zb], gg[...], preferred_element_type=F32)
        last = jnp.dot(got[zb], hp[...], preferred_element_type=F32)
        for t in range(8):
            if t < 5:
                column = pair[:, 128 * t:128 * t + 128]
            elif t == 5:
                column = pair[:, 640:768] + last[:, 0:128]
            else:
                column = last[:, 128 * (t - 5):128 * (t - 4)]
            gb[zb, :, :, HALF * t:HALF * t + HALF, :] = column.astype(BF16).reshape(NY, NC, HALF, 128)
        gb[zb, :, :, 256:PACK, :] = folded(last[:, 384:512]).astype(BF16).reshape(NY, NC, 8, 128)
        remote(gb.at[zb, :, 1 - c], gr.at[zb], gift_s, gift_r.at[EZ.index(ez)], {"c": 1 - c})

    gifted = set()

    def add_up(n, store):
        ez, _ = n
        if ez not in gifted:
            expect(gr.at[at("z", -ez)], gift_r.at[EZ.index(ez)])
            gifted.add(ez)
        kids = [(m, rows_of(m)) for m in sends_of(n)]
        for m, (a, b) in kids:
            expect(r.at[m[0] + 4, m[1] + 2, pl.ds(a, b - a)], rs_r.at[ids[m]])
        edges = sorted({0, PACK, *(v for _, ab in kids for v in ab)})
        zb, yb = at("z", -ez), at("y", -n[1])
        for a, b in zip(edges, edges[1:]):
            total = gb[zb, yb, c, a:b, :].astype(F32) + gr[zb, yb, a:b, :].astype(F32)
            for m, (ka, kb) in kids:
                if ka <= a and b <= kb:
                    total = total + r[m[0] + 4, m[1] + 2, a:b, :].astype(F32)
            store(a, b, total)

    def give(n):
        sz, sy = n[0] + 4, n[1] + 2

        def store(a, b, total):
            s[sz, sy, a:b, :] = total.astype(BF16)

        add_up(n, store)
        for m in parts_of(n):
            a, b = rows_of(m)
            axis, step = step_of(m)
            piece = s.at[sz, sy, pl.ds(a, b - a)]
            if m[1] == 0 and abs(m[0]) <= 2:
                side = 0 if m[0] > 0 else 1
                remote(piece, far_sum.at[side, c], back_s, top_r.at[side, c], {"z": at("z", -step), "c": par})
            else:
                remote(
                    piece, r.at[m[0] + 4, m[1] + 2, pl.ds(a, b - a)], rs_s, rs_r.at[ids[m]],
                    {axis: at(axis, -step)},
                )

    outs = []

    def share(which, left, columns, zb):
        value = lax.dot_general(
            left[...], weights(zb, *columns),
            (((1,), (1,)), ((), ())), preferred_element_type=F32,
        ).astype(BF16).reshape(NB, TOKENS, ZB)
        part[which, :, :, ZB * zb:ZB * zb + ZB] = value
        if zb % 4 == 3:
            h = zb // 4
            over, under, across = at("x", 1), at("x", -1), at("x", 2)
            for i, (block, to) in enumerate((
                (across * NC, over), (over * NC + 1, over), (across * NC + 1, under), (under * NC, under),
            )):
                remote(
                    part.at[which, block, :, wide[h]], ring.at[which, i, :, wide[h]],
                    ring_s, ring_r.at[which, h, i], {"x": to},
                )

    wide = (pl.ds(0, 1024), pl.ds(1024, 1024))

    def share_on(which, h):
        for i, (at_ring, sign) in enumerate(((0, 1), (2, -1))):
            to = at("x", sign)
            expect(ring.at[which, at_ring, :, wide[h]], ring_r.at[which, h, at_ring])
            ringed[which, i, :, wide[h]] = (
                part[which, to * NC + i, :, wide[h]].astype(F32) + ring[which, at_ring, :, wide[h]].astype(F32)
            ).astype(BF16)
            remote(
                ringed.at[which, i, :, wide[h]], ring.at[which, 4 + i, :, wide[h]],
                ring_s, ring_r.at[which, h, 4 + i], {"x": to},
            )

    def share_plane(which, h):
        for i in (1, 3, 4, 5):
            expect(ring.at[which, i, :, wide[h]], ring_r.at[which, h, i])
        for q, (i, k) in enumerate(((3, 4), (1, 5))):
            plane[which, q, :, wide[h]] = (
                part[which, x * NC + q, :, wide[h]].astype(F32)
                + ring[which, i, :, wide[h]].astype(F32) + ring[which, k, :, wide[h]].astype(F32)
            ).astype(BF16)

        @pl.when(moves)
        def _():
            for q in range(NC):
                remote(
                    plane.at[which, q, :, wide[h]], crossed.at[which, 0, :, wide[h]],
                    plane_s, plane_r.at[which, h, 0], {"z": zp, "c": q},
                )

        @pl.when(keeps)
        def _():
            remote(
                plane.at[which, 1 - c, :, wide[h]], crossed.at[which, 1, :, wide[h]],
                plane_s, plane_r.at[which, h, 1], {"c": 1 - c},
            )

    def put(src, dst, i):
        pltpu.make_async_copy(src, dst, out_s.at[i]).start()

    def share_final(which, out):
        for h in range(2):
            expect(crossed.at[which, 0, :, wide[h]], plane_r.at[which, h, 0])

        @pl.when(keeps)
        def _():
            outv[which] = (plane[which, c].astype(F32) + crossed[which, 0].astype(F32)).astype(BF16)

        @pl.when(moves)
        def _():
            for h in range(2):
                expect(crossed.at[which, 1, :, wide[h]], plane_r.at[which, h, 1])
            outv[which] = (crossed[which, 1].astype(F32) + crossed[which, 0].astype(F32)).astype(BF16)

        put(outv.at[which], out, which)

    def forward_gate():
        gate = known(accn[...])
        upper = known(pltpu.roll(accn[...], 768 - UNITS, 1))
        value = gate * (1.0 / (1.0 + jnp.exp(-gate))) * upper
        hid[...] = value.astype(BF16)
        hidp[...] = packed_last(value).astype(BF16)

        @pl.when(keeps)
        def _():
            put(hid, hid_ref, 2)

        @pl.when(moves)
        def _():
            remote(hid, hidv, hid_s, hid_r, {"z": zp, "c": 1 - c})

    def hidden_out():
        @pl.when(moves)
        def _():
            expect(hidv, hid_r)
            put(hidv, hid_ref, 2)

    def next_blocks(ezs):
        for ez in ezs:
            project(2, accn, (0, 6), at("z", -ez), ez == 0)

    def share_in(zb):
        share(1, gg, (0, 6), zb)

    def share_next(zb):
        share(0, hidp, (5, 9), zb)

    plan = [(0, share_in, 0)] + [(3 + (i - 1) // 2, share_in, i) for i in range(1, NZ)]
    plan += [(7, tok_far, 2), (7, next_blocks, EZ[0:4]), (8, next_blocks, EZ[4:8]), (9, forward_gate)]
    plan += [(9, share_next, 0), (9, share_on, 1, 0), (10, share_next, 1), (10, share_next, 2), (11, share_next, 3)]
    plan += [(11, share_next, 4), (12, share_next, 5), (12, share_on, 1, 1), (13, share_next, 6), (13, share_next, 7)]
    plan += [
        (20, share_plane, 1, 0), (22, share_on, 0, 0), (25, share_plane, 1, 1), (29, share_on, 0, 1),
        (29, hidden_out), (29, share_plane, 0, 0), (31, share_plane, 0, 1),
        (92, share_final, 1, gin_ref), (93, share_final, 0, out_ref),
    ]

    def between(until):
        while plan and plan[0][0] <= until:
            _, work, *given = plan.pop(0)
            with jax.named_scope("w#%s" % "_".join([work.__name__] + [str(v) for v in given if isinstance(v, int)])):
                work(*given)

    graded = set()
    for count, n in enumerate(REDUCE):
        for e in (abs(n[0]), abs(n[0]) - 1):
            if e >= 0 and e not in graded:
                with jax.named_scope("wgrad#e=%d" % e):
                    for ez in block_steps(e):
                        weight_grad(ez)
                graded.add(e)
        between(count)
        with jax.named_scope("give#i=%d#z=%d#y=%d" % (count, *n)):
            give(n)
        between(count + 1)

    with jax.named_scope("last"):

        @pl.when(moves)
        def _():
            home[...] = jnp.zeros((NC, PACK, 128), F32)

        def keep(a, b, total):
            home_in[0, a:b, :] = total.astype(BF16)

            @pl.when(keeps)
            def _():
                home[c, a:b, :] = total

        add_up((0, 0), keep)

        @pl.when(moves)
        def _():
            remote(home_in.at[0], home_in.at[1], home_s, home_r, {"c": 1 - c})

    between(99)
    with jax.named_scope("final"):

        @pl.when(keeps)
        def _():
            expect(home_in.at[1], home_r)
            home[1 - c] = home_in[1].astype(F32)

        for side in range(2):
            for q in range(NC):
                expect(far_sum.at[side, q], top_r.at[side, q])
        for q in range(NC):
            home[q] = (
                home[q] + far_sum[0, q].astype(F32) + far_sum[1, q].astype(F32)
            )
            put(home.at[q], wg_out.at[q], 3 + q)
    with jax.named_scope("drain"):
        routed = sum(rows_of(m)[1] - rows_of(m)[0] for m in ids if m[1] or abs(m[0]) > 2) // PACK
        for count, sem in ((routed, ag_s), (routed, rs_s), (4, top_s), (4, back_s), (NZ * NY - 1, twin_s)):
            expect(w.at[pl.ds(0, count), 0], sem)
        expect(gr, gift_s)
        for count, sem in ((18, tk_s), (12, ring_s)):
            expect(tok.at[pl.ds(0, count)], sem)

        @pl.when(keeps)
        def _():
            expect(own, home_s)
            expect(tok.at[pl.ds(0, 3)], hop_s)
            expect(tok.at[pl.ds(0, 2)], plane_s)

        @pl.when(moves)
        def _():
            expect(home_in.at[0], home_s)
            expect(tok.at[pl.ds(0, 6)], hop_s)
            expect(tok.at[pl.ds(0, 4)], plane_s)
            expect(hid, hid_s)

        for i, (src, dst) in enumerate(((outv.at[0], out_ref), (outv.at[1], gin_ref), (hid, hid_ref), *((home.at[q], wg_out.at[q]) for q in range(NC)))):
            pltpu.make_async_copy(src, dst, out_s.at[i]).wait()


def finish(
    factor, out_in, hid_in, gin_in, wg_in, ag_in, au_in, ad_in,
    out_ref, hid_ref, gin_ref, ng_ref, nu_ref, nd_ref, hidv, wg, ag, au, ad, sems,
):
    pairs = ((wg_in, wg), (out_in, out_ref), (gin_in, gin_ref), (hid_in, hidv), (ag_in, ag), (au_in, au), (ad_in, ad))
    copies = [pltpu.make_async_copy(src, dst, sems.at[i]) for i, (src, dst) in enumerate(pairs)]
    for copy in copies:
        copy.start()
    for copy in copies:
        copy.wait()
    hid_ref[...] = hidv[:, 0:UNITS]
    for q in range(NC):
        column = [wg[q, HALF * t:HALF * t + HALF, :] for t in range(8)]
        tail = unfolded(wg[q, 256:PACK, :])
        gate = jnp.concatenate(column[0:3], axis=1)
        upper = pltpu.roll(jnp.concatenate(column[2:6], axis=1), 416, 1)
        down = pltpu.roll(jnp.concatenate(column[5:8] + [tail], axis=1), 448, 1)
        half = slice(HALF * q, HALF * q + HALF)
        for acc, new, value in ((ag, ng_ref, gate), (au, nu_ref, upper), (ad, nd_ref, down)):
            new[half, :] = acc[half, :] + factor * value[:, 0:UNITS]


def local(x_next, x_prev, grad_out, gate_w, up_w, down_w, acc_gate, acc_up, acc_down):
    _, ids = gather_plan()
    vmem = pl.BlockSpec(memory_space=pltpu.VMEM)
    hbm = pl.BlockSpec(memory_space=pl.ANY)
    dma = pltpu.SemaphoreType.DMA
    total_rows = x_prev.shape[0] * NZ * NY * NX * NC
    factor = 1.0 / math.sqrt(total_rows)
    rows = jax.ShapeDtypeStruct((TOKENS, 2048), BF16)
    out_next, hidden, grad_input, grads = pl.pallas_call(
        layer,
        out_shape=(
            rows, jax.ShapeDtypeStruct((GROUP, SEG), BF16), rows, jax.ShapeDtypeStruct((NC, PACK, 128), F32),
        ),
        in_specs=[hbm] * 6,
        out_specs=(hbm,) * 4,
        scratch_shapes=[
            pltpu.VMEM((3, TOKENS, 2048), BF16),
            pltpu.VMEM((3, ROWS, UNITS), BF16),
            pltpu.VMEM((NC, PACK, 128), BF16),
            pltpu.VMEM((NZ * NY, NC, PACK, 128), BF16),
            pltpu.VMEM((3 * NB, TOKENS, 2048), BF16),
            pltpu.VMEM((NZ, ZB, GROUP), BF16),
            pltpu.VMEM((NZ, ZB, GROUP), BF16),
            pltpu.VMEM((GROUP, 768), F32),
            pltpu.VMEM((GROUP, 512), F32),
            pltpu.VMEM((GROUP, 2 * SEG), F32),
            pltpu.VMEM((GROUP, 2 * SEG), BF16),
            pltpu.VMEM((GROUP, 512), BF16),
            pltpu.VMEM((GROUP, SEG), BF16),
            pltpu.VMEM((GROUP, 512), BF16),
            pltpu.VMEM((GROUP, SEG), BF16),
            pltpu.VMEM((NZ, NY, NC, PACK, 128), BF16),
            pltpu.VMEM((NZ, NY, PACK, 128), BF16),
            pltpu.VMEM((9, 5, PACK, 128), BF16),
            pltpu.VMEM((9, 5, PACK, 128), BF16),
            pltpu.VMEM((2, NC, PACK, 128), BF16),
            pltpu.VMEM((2, PACK, 128), BF16),
            pltpu.VMEM((NC, PACK, 128), F32),
            pltpu.VMEM((2, NB, TOKENS, 2048), BF16),
            pltpu.VMEM((2, 6, TOKENS, 2048), BF16),
            pltpu.VMEM((2, 2, TOKENS, 2048), BF16),
            pltpu.VMEM((2, NC, TOKENS, 2048), BF16),
            pltpu.VMEM((2, NC, TOKENS, 2048), BF16),
            pltpu.VMEM((2, TOKENS, 2048), BF16),
            dma, dma((len(ids),)), dma, dma, dma, dma((len(EZ),)), dma, dma((3, NC)), dma, dma((3, 4)),
            dma, dma((len(EZ),)), dma, dma((len(ids),)), dma, dma((2, NC)), dma, dma,
            dma, dma((2, 2, 6)), dma, dma((2, 2, 2)),
            dma, dma, dma((5,)), dma((6,)),
        ],
        compiler_params=pltpu.CompilerParams(
            collective_id=0, has_side_effects=True, vmem_limit_bytes=60 * 1024 * 1024
        ),
        name="layer",
    )(x_next, x_prev, grad_out, gate_w, up_w, down_w.T)
    sums = jax.ShapeDtypeStruct((ROWS, UNITS), F32)
    out_next, hidden, grad_input, new_gate, new_up, new_down = pl.pallas_call(
        functools.partial(finish, factor),
        out_shape=(rows, jax.ShapeDtypeStruct((GROUP, UNITS), BF16), rows, sums, sums, sums),
        in_specs=[hbm] * 7,
        out_specs=(vmem,) * 6,
        scratch_shapes=[pltpu.VMEM((GROUP, SEG), BF16), pltpu.VMEM((NC, PACK, 128), F32)]
        + [pltpu.VMEM((ROWS, UNITS), F32)] * 3 + [dma((7,))],
        compiler_params=pltpu.CompilerParams(vmem_limit_bytes=60 * 1024 * 1024),
        name="finish",
    )(out_next, hidden, grad_input, grads, acc_gate, acc_up, acc_down.T)
    return out_next, hidden, grad_input, new_gate, new_up, new_down.T


def solution(mesh):
    split = Mesh(mesh.devices.reshape(NZ, NY, NX, NC), ("z", "y", "x", "c"))
    in_specs = (
        P(TOK, None), P(TOK, None), P(TOK, None),
        P(FS, TP), P(FS, TP), P(TP, FS), P(FS, TP), P(FS, TP), P(TP, FS),
    )
    out_specs = (P(TOK, None), P(FS, TP), P(TOK, None), P(FS, TP), P(FS, TP), P(TP, FS))
    return jax.shard_map(local, mesh=split, in_specs=in_specs, out_specs=out_specs, check_vma=False)
```
